128 devices in a mesh: sp: 16 (over z, y), tp: 8 (over x, core).
Axes of the slice: x: 4, y: 4, z: 4, core: 2. Of those that a mesh axis runs over, the one named last changes fastest.
Arguments:
- values_in: bfloat16 [4, 16384, 1024], P(None, 'sp', 'tp'), may hold values from -6 to 6
- gates_in: bfloat16 [4, 16384, 1024], P(None, 'sp', 'tp'), may hold values from -8 to 8
- conv_taps: bfloat16 [31, 1024], P(None, 'tp'), may hold values from -3 to 3
- conv_bias: bfloat16 [1024], P('tp'), may hold values from -3 to 3
- norm_gain: bfloat16 [1024], P('tp'), may hold values from 0.099609375 to 1.8984375
- out_weight: bfloat16 [1024, 4096], P('tp'), may hold values from -0.1875 to 0.1875
- out_grad: bfloat16 [4, 16384, 4096], P(None, 'sp'), may hold values from -1.5 to 1.5
Outputs:
- values_grad: bfloat16 [4, 16384, 1024], P(None, 'sp', 'tp')
- gates_grad: bfloat16 [4, 16384, 1024], P(None, 'sp', 'tp')
- taps_grad: float32 [31, 1024], P(None, 'tp')
- gain_grad: float32 [1024], P('tp')
- bias_grad: float32 [1024], P('tp')
- weight_grad: float32 [1024, 4096], P(('tp', 'sp'))
The draws below stay inside these ranges and needn't reach their ends.
All inputs are finite; a program needn't handle non-finite values.
Results may differ from the reference program's by a relative error of at most 0.0048.
Values may be sent and summed in bfloat16 or wider, within the bound.
No kernel may reach another device: no remote copies, remote signals or barrier semaphores. Data moves between devices by JAX's collectives and lax.ppermute only.
A program may use at most 128 MiB of HBM per device.

```python
import jax
import jax.numpy as jnp
from jax import lax

D = 4096
C = 1024
K = 31
SEQS = 4
TOKENS = 16384


def draw_conv_taps(key, part):
    normal_key, scale_key = jax.random.split(jax.random.fold_in(key, 7))
    group_count = C // 64
    scales = jnp.exp(jax.random.uniform(scale_key, (group_count,), jnp.float32, -1.2, 1.2))
    scales = jnp.repeat(scales, 64)
    noise = jax.random.normal(normal_key, (K, C), jnp.float32)
    noise = jnp.clip(noise, -4.0, 4.0)
    return (noise * scales[None, :] * K ** (-0.5)).astype(jnp.bfloat16)


def block_levels(key, shape, cuts, smallest, largest):
    def one(dim, blocks):
        draws = jax.random.uniform(jax.random.fold_in(jax.random.fold_in(key, 6), dim), (blocks,), jnp.float32, smallest / len(cuts), largest / len(cuts))
        return jnp.repeat(jnp.exp(draws), shape[dim] // blocks).reshape((-1,) + (1,) * (len(shape) - dim - 1))

    level = one(*cuts[0])
    for cut in cuts[1:]:
        level = level * one(*cut)
    return level


def normal_values(key, shape, spread, reach, cuts=(), held_as=jnp.bfloat16):
    level = block_levels(key, shape, cuts, -0.22, 0.18) if cuts else 1.0
    result = jax.random.normal(key, shape, jnp.float32) * spread * level
    return jnp.minimum(jnp.maximum(result, -reach), reach).astype(held_as)


def setup_inputs(seed: int = 0) -> dict:
    key_of = jax.random.split(jax.random.key(seed), 8)
    values_in = normal_values(key_of[0], (SEQS, TOKENS, C), 1.0, 6.0, ((1, 16), (2, 8)))
    gates_in = normal_values(key_of[1], (SEQS, TOKENS, C), 1.5, 8.0, ((1, 16), (2, 8)))
    conv_taps = draw_conv_taps(jax.random.fold_in(key_of[7], 71), 0)
    conv_bias = normal_values(key_of[3], (C,), 0.5, 3.0, ((0, 8),))
    norm_gain = jnp.clip(1.0 + 0.18 * jax.random.normal(key_of[4], (C,), jnp.float32), 0.099609375, 1.8984375).astype(jnp.bfloat16)
    out_weight = normal_values(key_of[5], (C, D), C ** -0.5, 0.1875, ((0, 8),))
    out_grad = normal_values(key_of[6], (SEQS, TOKENS, D), 0.25, 1.5, ((1, 16),))
    return {"values_in": values_in, "gates_in": gates_in, "conv_taps": conv_taps, "conv_bias": conv_bias, "norm_gain": norm_gain, "out_weight": out_weight, "out_grad": out_grad}


EPS = 1e-05

def reference(values_in, gates_in, conv_taps, conv_bias, norm_gain, out_weight, out_grad):
    sig = jax.nn.sigmoid(gates_in.astype(jnp.float32))
    gated = (values_in.astype(jnp.float32) * sig).astype(jnp.bfloat16)
    tap_rows = conv_taps.astype(jnp.float32)
    length = gated.shape[1]
    padded = jnp.pad(gated.astype(jnp.float32), ((0, 0), (K - 1, 0), (0, 0)))
    conv = jnp.zeros(gated.shape, jnp.float32) + conv_bias.astype(jnp.float32)
    for tap_index in range(K):
        conv = conv + tap_rows[tap_index] * padded[:, tap_index:tap_index + length]
    channel_mean = lax.optimization_barrier(jnp.mean(conv, axis=-1, keepdims=True))
    centered = conv - channel_mean
    variance = lax.optimization_barrier(jnp.mean(centered * centered, axis=-1, keepdims=True))
    inverse = lax.rsqrt(variance + EPS)
    normed = centered * inverse
    gain = norm_gain.astype(jnp.float32)
    scaled = normed * gain
    swished = jax.nn.silu(scaled).astype(jnp.bfloat16)
    flat_grad = out_grad.reshape(-1, D)
    weight_grad = jnp.dot(swished.reshape(-1, C).T, flat_grad, preferred_element_type=jnp.float32)
    swish_grad = jnp.dot(flat_grad, out_weight.T, preferred_element_type=jnp.float32).reshape(gated.shape)
    scaled_sig = jax.nn.sigmoid(scaled)
    scaled_grad = swish_grad * scaled_sig * (1.0 + scaled * (1.0 - scaled_sig))
    gain_grad = lax.optimization_barrier(jnp.sum(scaled_grad * normed, axis=(0, 1)))
    normed_grad = scaled_grad * gain
    conv_grad = inverse * (normed_grad - lax.optimization_barrier(jnp.mean(normed_grad, axis=-1, keepdims=True)) - normed * lax.optimization_barrier(jnp.mean(normed_grad * normed, axis=-1, keepdims=True)))
    bias_grad = lax.optimization_barrier(jnp.sum(conv_grad, axis=(0, 1)))
    taps_grad = jnp.stack([lax.optimization_barrier(jnp.sum(conv_grad * padded[:, tap_index:tap_index + length], axis=(0, 1))) for tap_index in range(K)])
    padded_grad = jnp.pad(conv_grad, ((0, 0), (0, K - 1), (0, 0)))
    gated_grad = jnp.zeros(gated.shape, jnp.float32)
    for tap_index in range(K):
        begin = K - 1 - tap_index
        gated_grad = gated_grad + tap_rows[tap_index] * padded_grad[:, begin:begin + length]
    values_grad = (gated_grad * sig).astype(jnp.bfloat16)
    gates_grad = (gated_grad * values_in.astype(jnp.float32) * sig * (1.0 - sig)).astype(jnp.bfloat16)
    return (values_grad, gates_grad, taps_grad, gain_grad, bias_grad, weight_grad)
```

```python
import functools

import jax
import jax.numpy as jnp
from jax import lax
from jax.experimental import pallas as pl
from jax.experimental.pallas import tpu as pltpu
from jax.sharding import PartitionSpec as P


K = 31
REACH = K - 1
PAD = 32
EPS = 1e-05
LANES = 128
F32 = jnp.float32
BF16 = jnp.bfloat16


def sigmoid(x):
    return 0.5 * jnp.tanh(0.5 * x) + 0.5


def taps_by_shift(first):
    groups = {}
    for tap in range(K):
        groups.setdefault(first(tap) % 8, []).append((tap, first(tap) // 8 * 8))
    return sorted(groups.items())


def conv_kernel(
    blocks, v_ref, g_ref, halo_ref, taps_ref, bias_ref,
    conv_ref, pay_ref, gated_ref, wide, tapf, rows,
):
    seq = pl.program_id(0)

    @pl.when(seq == 0)
    def _():
        tapf[:K] = taps_ref[...].astype(F32)

    gated_ref[0, :PAD] = halo_ref[0]
    wide[:PAD] = halo_ref[0].astype(F32)
    for b in range(blocks):
        at = b * LANES
        y = v_ref[0, at : at + LANES].astype(F32) * sigmoid(g_ref[0, at : at + LANES].astype(F32))
        y = y.astype(BF16)
        gated_ref[0, PAD + at : PAD + at + LANES] = y
        wide[PAD + at : PAD + at + LANES] = y.astype(F32)
    bias = bias_ref[...].astype(F32)

    def block(b, carry):
        at = b * LANES
        acc = jnp.broadcast_to(bias, (LANES, LANES))
        for shift, taps in taps_by_shift(lambda tap: tap + PAD - REACH):
            piece = wide[pl.ds(at + shift, LANES + taps[-1][1]), :]
            for tap, skip in taps:
                acc = acc + tapf[tap : tap + 1] * piece[skip : skip + LANES]
        turned = acc.T
        conv_ref[:, pl.ds(pl.multiple_of(at, LANES), LANES)] = turned
        mean = jnp.sum(turned, axis=0, keepdims=True) * (1.0 / LANES)
        off = turned - mean
        row = seq * blocks + b
        rows[pl.ds(row, 1)] = mean
        rows[pl.ds(row + rows.shape[0] // 2, 1)] = jnp.sum(off * off, axis=0, keepdims=True)
        return carry

    lax.fori_loop(0, blocks, block, 0, unroll=4)

    @pl.when(seq == pl.num_programs(0) - 1)
    def _():
        for peer in range(pay_ref.shape[0]):
            pay_ref[peer] = rows[...]


def swish_kernel(
    core_ref, w_hbm, w2_hbm, og_hbm, after_ref, mine_hbm, other_hbm,
    lhs, og, mine, other, wsem, sems, osems,
):
    n, tok, _ = og.shape
    chans = mine.shape[0]
    base = core_ref[0] * (n * tok)
    ins = []
    for i in range(n):
        at = pl.multiple_of(base + i * tok, tok)
        ins.append(pltpu.make_async_copy(og_hbm.at[pl.ds(at, tok)], og.at[i], sems.at[i]))
    weights = [
        pltpu.make_async_copy(w_hbm, lhs.at[pl.ds(0, chans)], wsem.at[0]),
        pltpu.make_async_copy(w2_hbm, lhs.at[pl.ds(chans, chans)], wsem.at[1]),
    ]
    for c in weights + ins:
        c.start()
    for c in weights:
        c.wait()
    outs = []
    for i in range(n):
        ins[i].wait()
        here = pl.ds(i * tok, tok)
        out = lax.dot_general(
            lhs[...], og[i], (((1,), (1,)), ((), ())), preferred_element_type=F32
        )
        mine[:, here] = out[:chans]
        other[:, here] = out[chans:].astype(BF16)
        outs += [
            pltpu.make_async_copy(mine.at[:, here], mine_hbm.at[:, here], osems.at[2 * i]),
            pltpu.make_async_copy(other.at[:, here], other_hbm.at[:, here], osems.at[2 * i + 1]),
        ]
        for c in outs[-2:]:
            c.start()
    for c in outs:
        c.wait()


def norm_kernel(
    core_ref, conv_ref, mine_ref, other_ref, got_ref, gain_ref,
    sw_ref, ng_ref, pay_ref, stat_ref, gg_ref, gcol, gacc, rows,
):
    step = pl.program_id(0)
    half = rows.shape[0] // 2
    peers = got_ref.shape[0]

    @pl.when(step == 0)
    def _():
        gain = jnp.broadcast_to(gain_ref[...].astype(F32), (LANES, LANES))
        gcol[...] = gain.T
        gacc[...] = jnp.zeros_like(gacc)
        mean = got_ref[0, :half]
        m2 = got_ref[0, half:]
        for p in range(1, peers):
            mean = mean + got_ref[p, :half]
            m2 = m2 + got_ref[p, half:]
        mean = mean * (1.0 / peers)
        apart = jnp.square(got_ref[0, :half] - mean)
        for p in range(1, peers):
            apart = apart + jnp.square(got_ref[p, :half] - mean)
        var = (m2 + LANES * apart) * (1.0 / (peers * LANES))
        stat_ref[:half] = mean
        stat_ref[half:] = lax.rsqrt(var + EPS)

    chunk = 32
    steps = pl.num_programs(0)
    seq = lax.rem(step + core_ref[0] * (steps // 2), steps)
    is_mine = step < steps // 2
    for j in range(conv_ref.shape[1] // LANES):
        at = j * LANES
        row = seq * (conv_ref.shape[1] // LANES) + j
        mean = stat_ref[pl.ds(row, 1)]
        inverse = stat_ref[pl.ds(half + row, 1)]
        s1 = jnp.zeros((8, LANES), F32)
        s2 = jnp.zeros((8, LANES), F32)
        for c in range(0, LANES, chunk):
            normed = (conv_ref[c : c + chunk, at : at + LANES] - mean) * inverse
            gain = gcol[c : c + chunk]
            scaled = normed * gain
            sig = sigmoid(scaled)
            sw_ref[c : c + chunk, at : at + LANES] = (scaled * sig).astype(BF16)
            swg = jnp.where(
                is_mine,
                mine_ref[c : c + chunk, at : at + LANES],
                other_ref[c : c + chunk, at : at + LANES].astype(F32),
            )
            sg = swg * sig * (1.0 + scaled * (1.0 - sig))
            gacc[c : c + chunk] += sg * normed
            ng = sg * gain
            ng_ref[c : c + chunk, at : at + LANES] = ng
            nn = ng * normed
            for r in range(0, chunk, 8):
                s1 = s1 + ng[r : r + 8]
                s2 = s2 + nn[r : r + 8]
        rows[pl.ds(row, 1)] = jnp.sum(s1, axis=0, keepdims=True)
        rows[pl.ds(half + row, 1)] = jnp.sum(s2, axis=0, keepdims=True)

    @pl.when(step == pl.num_programs(0) - 1)
    def _():
        gg_ref[...] = jnp.sum(gacc[...].T, axis=0, keepdims=True)
        for peer in range(peers):
            pay_ref[peer] = rows[...]


def weight_kernel(
    core_ref, sw_hbm, sw2_hbm, og_hbm, mine_hbm, other_hbm, lhs, og, mine, other, wsem, sems, osems
):
    n, _, cols = og.shape
    chans = lhs.shape[0] // 2
    base = core_ref[0] * (n * cols)
    ins = []
    for i in range(n):
        at = pl.multiple_of(base + i * cols, cols)
        ins.append(pltpu.make_async_copy(og_hbm.at[:, pl.ds(at, cols)], og.at[i], sems.at[i]))
    sides = [
        pltpu.make_async_copy(sw_hbm, lhs.at[pl.ds(0, chans)], wsem.at[0]),
        pltpu.make_async_copy(sw2_hbm, lhs.at[pl.ds(chans, chans)], wsem.at[1]),
    ]
    for c in sides + ins:
        c.start()
    for c in sides:
        c.wait()
    outs = []
    for i in range(n):
        ins[i].wait()
        part = jnp.dot(lhs[...], og[i], preferred_element_type=F32).astype(BF16)
        mine[i] = part[:chans].reshape(mine.shape[1:])
        other[i] = part[chans:].reshape(other.shape[1:])
        here = pl.ds(i * cols, cols)
        outs += [
            pltpu.make_async_copy(mine.at[i], mine_hbm.at[:, :, here], osems.at[2 * i]),
            pltpu.make_async_copy(other.at[i], other_hbm.at[:, :, here], osems.at[2 * i + 1]),
        ]
        for c in outs[-2:]:
            c.start()
    for c in outs:
        c.wait()


def turn_kernel(
    blocks, conv_ref, ng_ref, stat_ref, got_ref, cg_ref, head_ref, bias_ref, bias_acc, means
):
    seq = pl.program_id(0)
    half = stat_ref.shape[0] // 2
    peers = got_ref.shape[0]
    total = peers * LANES

    @pl.when(seq == 0)
    def _():
        s = got_ref[0]
        for p in range(1, peers):
            s = s + got_ref[p]
        means[...] = s * (1.0 / total)
        bias_acc[...] = jnp.zeros_like(bias_acc)

    for b in range(blocks):
        here = slice(b * LANES, (b + 1) * LANES)
        row = seq * blocks + b
        mean = stat_ref[pl.ds(row, 1)]
        inverse = stat_ref[pl.ds(half + row, 1)]
        m1 = means[pl.ds(row, 1)]
        m2 = means[pl.ds(half + row, 1)]
        normed = (conv_ref[:, here] - mean) * inverse
        cg = inverse * (ng_ref[:, here] - m1 - normed * m2)
        cg = cg.T
        cg_ref[0, here, :] = cg
        part = cg[:8]
        for r in range(8, LANES, 8):
            part = part + cg[r : r + 8]
        bias_acc[...] += part
        if b == 0:
            head_ref[0] = cg[:PAD]

    @pl.when(seq == pl.num_programs(0) - 1)
    def _():
        bias_ref[...] = jnp.sum(bias_acc[...], axis=0, keepdims=True)


def taps_kernel(
    blocks, cg_ref, gated_ref, gg_ref, bias_ref, got_hbm, pay_in,
    pay_ref, wide, taps_acc, small, came, sem, csems,
):
    seq = pl.program_id(0)
    at = came.shape[2]
    take = pltpu.make_async_copy(got_hbm, came, csems.at[0])
    put = pltpu.make_async_copy(came, pay_ref.at[:, :, pl.ds(at, at)], csems.at[1])

    @pl.when(seq == 0)
    def _():
        take.start()
        taps_acc[...] = jnp.zeros_like(taps_acc)

    @pl.when(seq == 1)
    def _():
        take.wait()
        put.start()

    wide[...] = gated_ref[0].astype(F32)

    def block(b, carry):
        at = b * LANES
        cg = cg_ref[0, pl.ds(pl.multiple_of(at, LANES), LANES), :]
        for shift, taps in taps_by_shift(lambda tap: tap + PAD - REACH):
            piece = wide[pl.ds(at + shift, LANES + taps[-1][1]), :]
            for tap, skip in taps:
                acc = taps_acc[tap]
                for r in range(0, LANES, 8):
                    acc = acc + cg[r : r + 8] * piece[skip + r : skip + r + 8]
                taps_acc[tap] = acc
        return carry

    lax.fori_loop(0, blocks, block, 0, unroll=2)

    @pl.when(seq == pl.num_programs(0) - 1)
    def _():
        rows = [jnp.sum(taps_acc[tap], axis=0, keepdims=True) for tap in range(K)]
        rows += [gg_ref[...], bias_ref[...]]
        rows += [jnp.zeros((1, LANES), F32)] * (-len(rows) % 8)
        for t in range(len(rows) // 8):
            tile = jnp.concatenate(rows[8 * t : 8 * t + 8], axis=0).astype(BF16)
            for peer in range(small.shape[0]):
                small[peer, :, t * LANES : (t + 1) * LANES] = tile
        copy = pltpu.make_async_copy(
            small, pay_ref.at[:, :, pl.ds(2 * at, small.shape[2])], sem
        )
        copy.start()
        copy.wait()
        put.wait()


def spread_kernel(blocks, cg_ref, next_ref, v_ref, g_ref, taps_ref, vg_ref, gg_ref, wide, tapf):
    @pl.when(pl.program_id(0) == 0)
    def _():
        tapf[:K] = taps_ref[...].astype(F32)

    length = blocks * LANES
    wide[:length] = cg_ref[0]
    wide[length : length + PAD] = next_ref[0]

    def block(b, carry):
        at = b * LANES
        acc = None
        for shift, taps in taps_by_shift(lambda tap: REACH - tap):
            piece = wide[pl.ds(at + shift, LANES + max(skip for _, skip in taps)), :]
            for tap, skip in taps:
                term = tapf[tap : tap + 1] * piece[skip : skip + LANES]
                acc = term if acc is None else acc + term
        here = pl.ds(pl.multiple_of(at, LANES), LANES)
        sig = sigmoid(g_ref[0, here, :].astype(F32))
        v = v_ref[0, here, :].astype(F32)
        vg = acc * sig
        vg_ref[0, here, :] = vg.astype(BF16)
        gg_ref[0, here, :] = (vg * v * (1.0 - sig)).astype(BF16)
        return carry

    lax.fori_loop(0, blocks, block, 0, unroll=4)


def final_kernel(core_ref, got_ref, w_ref, taps_ref, gain_ref, bias_ref):
    acc = got_ref[0].astype(F32)
    for p in range(1, got_ref.shape[0]):
        acc = acc + got_ref[p].astype(F32)
    width = w_ref.shape[1]
    half = width // 2
    for side in range(2):
        at = pl.multiple_of((core_ref[0] + side) % 2 * half, half)
        w_ref[:, pl.ds(at, half)] = acc[:, side * half : (side + 1) * half]
    for t in range(K // 8 + 1):
        tile = acc[:, width + t * LANES : width + (t + 1) * LANES]
        taps_ref[8 * t : min(8 * t + 8, K)] = tile[: min(8, K - 8 * t)]
    for ref, row in ((gain_ref, K), (bias_ref, K + 1)):
        at = width + row // 8 * LANES
        ref[...] = acc[row % 8 : row % 8 + 1, at : at + LANES]


def whole(shape):
    return pl.BlockSpec(shape, lambda i: (0,) * len(shape))


PARAMS = pltpu.CompilerParams(vmem_limit_bytes=67_000_000)


def cost(flops, moved):
    return pl.CostEstimate(flops=flops, bytes_accessed=moved, transcendentals=0)


def on_device(values_in, gates_in, conv_taps, conv_bias, norm_gain, out_weight, out_grad):
    seqs, length, chans = values_in.shape
    width = out_grad.shape[2]
    tokens = seqs * length
    blocks = length // LANES
    tp, sp = lax.axis_size("tp"), lax.axis_size("sp")
    stat_rows = 2 * tokens // LANES
    flat = out_grad.reshape(tokens, width)
    ahead = [(i, i + 1) for i in range(sp - 1)]
    back = [(i + 1, i) for i in range(sp - 1)]
    swap = [(i, i ^ 1) for i in range(tp)]
    core = (lax.axis_index("tp") % 2).astype(jnp.int32).reshape(1)
    bias_row = conv_bias.reshape(1, chans)
    gain_row = norm_gain.reshape(1, chans)

    SDS = jax.ShapeDtypeStruct
    any_ = pl.BlockSpec(memory_space=pl.ANY)
    vmem = pl.BlockSpec(memory_space=pltpu.VMEM)
    smem = pl.BlockSpec(memory_space=pltpu.SMEM)
    seq_block = pl.BlockSpec((1, length, chans), lambda i: (i, 0, 0))
    head_block = pl.BlockSpec((1, PAD, chans), lambda i: (i, 0, 0))
    gated_block = pl.BlockSpec((1, length + PAD, chans), lambda i: (i, 0, 0))
    col = pl.BlockSpec((chans, length), lambda i: (0, i))
    stats = whole((tp, stat_rows, LANES))

    tail = slice(length - PAD, length)
    edge = values_in[:, tail].astype(F32) * sigmoid(gates_in[:, tail].astype(F32))
    halo = lax.ppermute(edge.astype(BF16), "sp", ahead)
    weight2 = lax.ppermute(out_weight, "tp", swap)
    conv, pay, gated = pl.pallas_call(
        functools.partial(conv_kernel, blocks),
        grid=(seqs,),
        in_specs=[seq_block, seq_block, head_block, whole((K, chans)), whole((1, chans))],
        out_specs=[col, stats, gated_block],
        out_shape=[
            SDS((chans, tokens), F32),
            SDS((tp, stat_rows, LANES), F32),
            SDS((seqs, length + PAD, chans), BF16),
        ],
        scratch_shapes=[
            pltpu.VMEM((length + 2 * PAD, chans), F32),
            pltpu.VMEM((PAD, chans), F32),
            pltpu.VMEM((stat_rows, LANES), F32),
        ],
        compiler_params=PARAMS,
        cost_estimate=cost(2 * K * tokens * chans, 8 << 20),
        name="conv",
    )(values_in, gates_in, halo, conv_taps, bias_row)
    got = lax.all_to_all(pay, "tp", 0, 0, tiled=True)

    pieces = 4
    mine, other = pl.pallas_call(
        swish_kernel,
        in_specs=[smem, any_, any_, any_, any_],
        out_specs=[any_, any_],
        out_shape=[SDS((chans, tokens // 2), F32), SDS((chans, tokens // 2), BF16)],
        scratch_shapes=[
            pltpu.VMEM((2 * chans, width), BF16),
            pltpu.VMEM((pieces, tokens // 2 // pieces, width), BF16),
            pltpu.VMEM((chans, tokens // 2), F32),
            pltpu.VMEM((chans, tokens // 2), BF16),
            pltpu.SemaphoreType.DMA((2,)),
            pltpu.SemaphoreType.DMA((pieces,)),
            pltpu.SemaphoreType.DMA((2 * pieces,)),
        ],
        compiler_params=PARAMS,
        cost_estimate=cost(2 * tokens * chans * width, tokens * width),
        name="swish_grad",
    )(core, out_weight, weight2, flat, pay)
    other = lax.ppermute(other, "tp", swap)

    half = seqs // 2
    turned = pl.BlockSpec((chans, length), lambda i, c: (0, (i + c[0] * half) % seqs))
    swished, ng, pay2, stat, gg = pl.pallas_call(
        norm_kernel,
        grid_spec=pltpu.PrefetchScalarGridSpec(
            num_scalar_prefetch=1,
            grid=(seqs,),
            in_specs=[
                turned,
                pl.BlockSpec((chans, length), lambda i, c: (0, jnp.minimum(i, half - 1))),
                pl.BlockSpec((chans, length), lambda i, c: (0, jnp.maximum(i, half) - half)),
                pl.BlockSpec((tp, stat_rows, LANES), lambda i, c: (0, 0, 0)),
                pl.BlockSpec((1, chans), lambda i, c: (0, 0)),
            ],
            out_specs=[
                turned,
                turned,
                pl.BlockSpec((tp, stat_rows, LANES), lambda i, c: (0, 0, 0)),
                pl.BlockSpec((stat_rows, LANES), lambda i, c: (0, 0)),
                pl.BlockSpec((1, chans), lambda i, c: (0, 0)),
            ],
            scratch_shapes=[
                pltpu.VMEM((chans, LANES), F32),
                pltpu.VMEM((chans, LANES), F32),
                pltpu.VMEM((stat_rows, LANES), F32),
            ],
        ),
        out_shape=[
            SDS((chans, tokens), BF16),
            SDS((chans, tokens), F32),
            SDS((tp, stat_rows, LANES), F32),
            SDS((stat_rows, LANES), F32),
            SDS((1, chans), F32),
        ],
        compiler_params=PARAMS,
        cost_estimate=cost(30 * tokens * chans, 8 << 20),
        name="norm",
    )(core, conv, mine, other, got, gain_row)
    swished2 = lax.ppermute(swished, "tp", swap)
    got2 = lax.all_to_all(pay2, "tp", 0, 0, tiled=True)

    extra = -(-(K + 2) // 8) * LANES
    cols = width // 2 // pieces
    part = (sp, chans // sp, width // 2)
    pay3, other_w = pl.pallas_call(
        weight_kernel,
        in_specs=[smem, any_, any_, any_],
        out_specs=[any_, any_],
        out_shape=[SDS((sp, chans // sp, width + extra), BF16), SDS(part, BF16)],
        scratch_shapes=[
            pltpu.VMEM((2 * chans, tokens), BF16),
            pltpu.VMEM((pieces, tokens, cols), BF16),
            pltpu.VMEM((pieces, sp, chans // sp, cols), BF16),
            pltpu.VMEM((pieces, sp, chans // sp, cols), BF16),
            pltpu.SemaphoreType.DMA((2,)),
            pltpu.SemaphoreType.DMA((pieces,)),
            pltpu.SemaphoreType.DMA((2 * pieces,)),
        ],
        compiler_params=PARAMS,
        cost_estimate=cost(2 * tokens * chans * width, tokens * width),
        name="weight_grad",
    )(core, swished, swished2, flat)
    other_w = lax.ppermute(other_w, "tp", swap)

    cg, head, bias_local = pl.pallas_call(
        functools.partial(turn_kernel, blocks),
        grid=(seqs,),
        in_specs=[col, col, whole((stat_rows, LANES)), stats],
        out_specs=[seq_block, head_block, whole((1, chans))],
        out_shape=[
            SDS((seqs, length, chans), F32),
            SDS((seqs, PAD, chans), F32),
            SDS((1, chans), F32),
        ],
        scratch_shapes=[pltpu.VMEM((8, chans), F32), pltpu.VMEM((stat_rows, LANES), F32)],
        compiler_params=PARAMS,
        cost_estimate=cost(30 * tokens * chans, 8 << 20),
        name="conv_grad",
    )(conv, ng, stat, got2)
    after = lax.ppermute(head, "sp", back)

    pay3 = pl.pallas_call(
        functools.partial(taps_kernel, blocks),
        grid=(seqs,),
        in_specs=[seq_block, gated_block, whole((1, chans)), whole((1, chans)), any_, any_],
        out_specs=any_,
        out_shape=SDS(pay3.shape, BF16),
        scratch_shapes=[
            pltpu.VMEM((length + PAD, chans), F32),
            pltpu.VMEM((K, 8, chans), F32),
            pltpu.VMEM((sp, chans // sp, extra), BF16),
            pltpu.VMEM(part, BF16),
            pltpu.SemaphoreType.DMA,
            pltpu.SemaphoreType.DMA((2,)),
        ],
        input_output_aliases={5: 0},
        compiler_params=PARAMS,
        cost_estimate=cost(2 * K * tokens * chans, 8 << 20),
        name="taps_grad",
    )(cg, gated, gg, bias_local, other_w, pay3)
    got3 = lax.all_to_all(pay3, "sp", 0, 0, tiled=True)

    values_grad, gates_grad = pl.pallas_call(
        functools.partial(spread_kernel, blocks),
        grid=(seqs,),
        in_specs=[seq_block, head_block, seq_block, seq_block, whole((K, chans))],
        out_specs=[seq_block, seq_block],
        out_shape=[SDS((seqs, length, chans), BF16)] * 2,
        scratch_shapes=[pltpu.VMEM((length + 2 * PAD, chans), F32), pltpu.VMEM((PAD, chans), F32)],
        compiler_params=PARAMS,
        cost_estimate=cost(2 * K * tokens * chans, 8 << 20),
        name="gated_grad",
    )(cg, after, values_in, gates_in, conv_taps)

    weight_grad, taps_grad, gain_grad, bias_grad = pl.pallas_call(
        final_kernel,
        in_specs=[smem, vmem],
        out_specs=[vmem] * 4,
        out_shape=[
            SDS((chans // sp, width), F32),
            SDS((K, chans), F32),
            SDS((1, chans), F32),
            SDS((1, chans), F32),
        ],
        compiler_params=PARAMS,
        name="final_sum",
    )(core, got3)
    gain_grad, bias_grad = gain_grad.reshape(chans), bias_grad.reshape(chans)
    return values_grad, gates_grad, taps_grad, gain_grad, bias_grad, weight_grad


def solution(mesh):
    return jax.shard_map(
        on_device,
        mesh=mesh,
        in_specs=(
            P(None, "sp", "tp"),
            P(None, "sp", "tp"),
            P(None, "tp"),
            P("tp"),
            P("tp"),
            P("tp", None),
            P(None, "sp", None),
        ),
        out_specs=(
            P(None, "sp", "tp"),
            P(None, "sp", "tp"),
            P(None, "tp"),
            P("tp"),
            P("tp"),
            P(("tp", "sp"), None),
        ),
        check_vma=False,
    )
```

```python
import functools

import jax
import jax.numpy as jnp
from jax import lax
from jax.experimental import pallas as pl
from jax.experimental.pallas import tpu as pltpu
from jax.sharding import PartitionSpec as P


K = 31
REACH = K - 1
PAD = 32
EPS = 1e-05
LANES = 128
F32 = jnp.float32
BF16 = jnp.bfloat16


def sigmoid(x):
    return 0.5 * jnp.tanh(0.5 * x) + 0.5


def taps_by_shift(first):
    groups = {}
    for tap in range(K):
        groups.setdefault(first(tap) % 8, []).append((tap, first(tap) // 8 * 8))
    return sorted(groups.items())


def conv_kernel(
    blocks, core_ref, v_ref, g_ref, halo_ref, taps_ref, bias_ref, w_hbm, w2_hbm, og_hbm,
    conv_ref, pay_ref, gated_ref, mine_ref, other_ref, wide, tapf, rows, lhs, og, wsem, sems,
):
    seq = pl.program_id(0)
    n, tok, _ = og.shape
    chans = mine_ref.shape[0]
    base = core_ref[0] * (og_hbm.shape[0] // 2)

    def fetch(i):
        at = base + i // 2 * (blocks * LANES) + i % 2 * tok
        return pltpu.make_async_copy(
            og_hbm.at[pl.ds(pl.multiple_of(at, tok), tok)], og.at[i], sems.at[i]
        )

    weights = [
        pltpu.make_async_copy(w_hbm, lhs.at[pl.ds(0, chans)], wsem.at[0]),
        pltpu.make_async_copy(w2_hbm, lhs.at[pl.ds(chans, chans)], wsem.at[1]),
    ]

    @pl.when(seq == 0)
    def _():
        for c in weights:
            c.start()
        fetch(0).start()
        tapf[:K] = taps_ref[...].astype(F32)

    @pl.when(seq < n - 1)
    def _():
        fetch(seq + 1).start()

    gated_ref[0, :PAD] = halo_ref[0]
    wide[:PAD] = halo_ref[0].astype(F32)
    for b in range(blocks):
        at = b * LANES
        y = v_ref[0, at : at + LANES].astype(F32) * sigmoid(g_ref[0, at : at + LANES].astype(F32))
        y = y.astype(BF16)
        gated_ref[0, PAD + at : PAD + at + LANES] = y
        wide[PAD + at : PAD + at + LANES] = y.astype(F32)
    bias = bias_ref[...].astype(F32)

    def block(b, carry):
        at = b * LANES
        acc = jnp.broadcast_to(bias, (LANES, LANES))
        for shift, taps in taps_by_shift(lambda tap: tap + PAD - REACH):
            piece = wide[pl.ds(at + shift, LANES + taps[-1][1]), :]
            for tap, skip in taps:
                acc = acc + tapf[tap : tap + 1] * piece[skip : skip + LANES]
        turned = acc.T
        conv_ref[:, pl.ds(pl.multiple_of(at, LANES), LANES)] = turned
        mean = jnp.sum(turned, axis=0, keepdims=True) * (1.0 / LANES)
        off = turned - mean
        row = seq * blocks + b
        rows[pl.ds(row, 1)] = mean
        rows[pl.ds(row + rows.shape[0] // 2, 1)] = jnp.sum(off * off, axis=0, keepdims=True)
        return carry

    lax.fori_loop(0, blocks // 2, block, 0, unroll=4)

    @pl.when(seq == 0)
    def _():
        for c in weights:
            c.wait()

    fetch(seq).wait()
    out = lax.dot_general(lhs[...], og[seq], (((1,), (1,)), ((), ())), preferred_element_type=F32)
    mine_ref[...] = out[:chans]
    other_ref[...] = out[chans:].astype(BF16)
    for b in range(blocks // 2, blocks):
        block(b, 0)

    @pl.when(seq == pl.num_programs(0) - 1)
    def _():
        for peer in range(pay_ref.shape[0]):
            pay_ref[peer] = rows[...]


def swish_kernel(
    core_ref, w_hbm, w2_hbm, og_hbm, after_ref, mine_hbm, other_hbm,
    lhs, og, mine, other, wsem, sems, osems,
):
    n, tok, _ = og.shape
    chans = mine.shape[0]
    base = core_ref[0] * (2 * n * tok)
    ins = []
    for i in range(n):
        at = pl.multiple_of(base + (2 * i + 1) * tok, tok)
        ins.append(pltpu.make_async_copy(og_hbm.at[pl.ds(at, tok)], og.at[i], sems.at[i]))
    weights = [
        pltpu.make_async_copy(w_hbm, lhs.at[pl.ds(0, chans)], wsem.at[0]),
        pltpu.make_async_copy(w2_hbm, lhs.at[pl.ds(chans, chans)], wsem.at[1]),
    ]
    for c in weights + ins:
        c.start()
    for c in weights:
        c.wait()
    outs = []
    for i in range(n):
        ins[i].wait()
        here = pl.ds(i * tok, tok)
        out = lax.dot_general(
            lhs[...], og[i], (((1,), (1,)), ((), ())), preferred_element_type=F32
        )
        mine[:, here] = out[:chans]
        other[:, here] = out[chans:].astype(BF16)
        outs += [
            pltpu.make_async_copy(mine.at[:, here], mine_hbm.at[:, here], osems.at[2 * i]),
            pltpu.make_async_copy(other.at[:, here], other_hbm.at[:, here], osems.at[2 * i + 1]),
        ]
        for c in outs[-2:]:
            c.start()
    for c in outs:
        c.wait()


def norm_kernel(
    core_ref, conv_ref, mine_a, other_a, mine_b, other_b, got_ref, gain_ref,
    sw_ref, ng_ref, pay_ref, stat_ref, gg_ref, gcol, gacc, rows,
):
    step = pl.program_id(0)
    half = rows.shape[0] // 2
    peers = got_ref.shape[0]

    @pl.when(step == 0)
    def _():
        gain = jnp.broadcast_to(gain_ref[...].astype(F32), (LANES, LANES))
        gcol[...] = gain.T
        gacc[...] = jnp.zeros_like(gacc)
        mean = got_ref[0, :half]
        m2 = got_ref[0, half:]
        for p in range(1, peers):
            mean = mean + got_ref[p, :half]
            m2 = m2 + got_ref[p, half:]
        mean = mean * (1.0 / peers)
        apart = jnp.square(got_ref[0, :half] - mean)
        for p in range(1, peers):
            apart = apart + jnp.square(got_ref[p, :half] - mean)
        var = (m2 + LANES * apart) * (1.0 / (peers * LANES))
        stat_ref[:half] = mean
        stat_ref[half:] = lax.rsqrt(var + EPS)

    chunk = 32
    steps = pl.num_programs(0)
    seq = lax.rem(step + core_ref[0] * (steps // 2), steps)
    is_mine = step < steps // 2
    for j in range(conv_ref.shape[1] // LANES):
        at = j * LANES
        row = seq * (conv_ref.shape[1] // LANES) + j
        late = at >= mine_a.shape[1]
        mine_ref, other_ref = (mine_b, other_b) if late else (mine_a, other_a)
        near = at - mine_a.shape[1] if late else at
        mean = stat_ref[pl.ds(row, 1)]
        inverse = stat_ref[pl.ds(half + row, 1)]
        s1 = jnp.zeros((8, LANES), F32)
        s2 = jnp.zeros((8, LANES), F32)
        for c in range(0, LANES, chunk):
            normed = (conv_ref[c : c + chunk, at : at + LANES] - mean) * inverse
            gain = gcol[c : c + chunk]
            scaled = normed * gain
            sig = sigmoid(scaled)
            sw_ref[c : c + chunk, at : at + LANES] = (scaled * sig).astype(BF16)
            swg = jnp.where(
                is_mine,
                mine_ref[c : c + chunk, near : near + LANES],
                other_ref[c : c + chunk, near : near + LANES].astype(F32),
            )
            sg = swg * sig * (1.0 + scaled * (1.0 - sig))
            gacc[c : c + chunk] += sg * normed
            ng = sg * gain
            ng_ref[c : c + chunk, at : at + LANES] = ng
            nn = ng * normed
            for r in range(0, chunk, 8):
                s1 = s1 + ng[r : r + 8]
                s2 = s2 + nn[r : r + 8]
        rows[pl.ds(row, 1)] = jnp.sum(s1, axis=0, keepdims=True)
        rows[pl.ds(half + row, 1)] = jnp.sum(s2, axis=0, keepdims=True)

    @pl.when(step == pl.num_programs(0) - 1)
    def _():
        gg_ref[...] = jnp.sum(gacc[...].T, axis=0, keepdims=True)
        for peer in range(peers):
            pay_ref[peer] = rows[...]


def weight_kernel(sw_ref, og_hbm, out_hbm, og, out, sems, osems):
    n, _, cols = og.shape
    ins = [
        pltpu.make_async_copy(og_hbm.at[:, pl.ds(i * cols, cols)], og.at[i], sems.at[i])
        for i in range(n)
    ]
    outs = [
        pltpu.make_async_copy(out.at[i], out_hbm.at[:, :, pl.ds(i * cols, cols)], osems.at[i])
        for i in range(n)
    ]
    for c in ins:
        c.start()
    for i in range(n):
        ins[i].wait()
        part = jnp.dot(sw_ref[...], og[i], preferred_element_type=F32)
        out[i] = part.astype(BF16).reshape(out.shape[1:])
        outs[i].start()
    for c in outs:
        c.wait()


def grad_kernel(
    blocks, conv_ref, ng_ref, stat_ref, got_ref, gated_ref, gg_ref, sw_ref, og_hbm, pay_in,
    cg_ref, head_ref, pay_ref,
    wide, taps_acc, bias_acc, means, small, og, out, sem, sems, osems,
):
    seq = pl.program_id(0)
    n, _, cols = og.shape

    def fetch(i):
        at = pl.multiple_of((n + i) * cols, LANES)
        return pltpu.make_async_copy(og_hbm.at[:, pl.ds(at, cols)], og.at[i], sems.at[i])

    def send(i):
        at = pl.multiple_of((n + i) * cols, LANES)
        return pltpu.make_async_copy(out.at[i], pay_ref.at[:, :, pl.ds(at, cols)], osems.at[i])

    @pl.when(seq == 0)
    def _():
        fetch(0).start()

    @pl.when(seq < n - 1)
    def _():
        fetch(seq + 1).start()

    half = stat_ref.shape[0] // 2
    peers = got_ref.shape[0]
    total = peers * LANES

    @pl.when(seq == 0)
    def _():
        s = got_ref[0]
        for p in range(1, peers):
            s = s + got_ref[p]
        means[...] = s * (1.0 / total)
        bias_acc[...] = jnp.zeros_like(bias_acc)
        taps_acc[...] = jnp.zeros_like(taps_acc)

    wide[...] = gated_ref[0].astype(F32)

    def block(b, carry):
        at = b * LANES
        here = pl.ds(pl.multiple_of(at, LANES), LANES)
        row = seq * blocks + b
        mean = stat_ref[pl.ds(row, 1)]
        inverse = stat_ref[pl.ds(half + row, 1)]
        m1 = means[pl.ds(row, 1)]
        m2 = means[pl.ds(half + row, 1)]
        normed = (conv_ref[:, here] - mean) * inverse
        cg = inverse * (ng_ref[:, here] - m1 - normed * m2)
        cg = cg.T
        cg_ref[0, here, :] = cg
        part = cg[:8]
        for r in range(8, LANES, 8):
            part = part + cg[r : r + 8]
        bias_acc[...] += part
        for shift, taps in taps_by_shift(lambda tap: tap + PAD - REACH):
            piece = wide[pl.ds(at + shift, LANES + taps[-1][1]), :]
            for tap, skip in taps:
                acc = taps_acc[tap]
                for r in range(0, LANES, 8):
                    acc = acc + cg[r : r + 8] * piece[skip + r : skip + r + 8]
                taps_acc[tap] = acc
        return carry

    lax.fori_loop(0, blocks // 2, block, 0, unroll=2)
    fetch(seq).wait()
    out[seq] = (
        jnp.dot(sw_ref[...], og[seq], preferred_element_type=F32)
        .astype(BF16)
        .reshape(out.shape[1:])
    )
    for b in range(blocks // 2, blocks // 2 + 2):
        block(b, 0)
    lax.fori_loop(blocks // 2 + 2, blocks, block, 0, unroll=2)
    send(seq).start()
    head_ref[0] = cg_ref[0, :PAD]

    @pl.when(seq == pl.num_programs(0) - 1)
    def _():
        rows = [jnp.sum(taps_acc[tap], axis=0, keepdims=True) for tap in range(K)]
        rows += [gg_ref[...], jnp.sum(bias_acc[...], axis=0, keepdims=True)]
        rows += [jnp.zeros((1, LANES), F32)] * (-len(rows) % 8)
        for t in range(len(rows) // 8):
            tile = jnp.concatenate(rows[8 * t : 8 * t + 8], axis=0).astype(BF16)
            for peer in range(small.shape[0]):
                small[peer, :, t * LANES : (t + 1) * LANES] = tile
        copy = pltpu.make_async_copy(
            small, pay_ref.at[:, :, pl.ds(2 * n * cols, small.shape[2])], sem
        )
        copy.start()
        copy.wait()
        for i in range(n):
            send(i).wait()


def spread_kernel(blocks, cg_ref, next_ref, v_ref, g_ref, taps_ref, vg_ref, gg_ref, wide, tapf):
    @pl.when(pl.program_id(0) == 0)
    def _():
        tapf[:K] = taps_ref[...].astype(F32)

    length = blocks * LANES
    wide[:length] = cg_ref[0]
    wide[length : length + PAD] = next_ref[0]

    def block(b, carry):
        at = b * LANES
        acc = None
        for shift, taps in taps_by_shift(lambda tap: REACH - tap):
            piece = wide[pl.ds(at + shift, LANES + max(skip for _, skip in taps)), :]
            for tap, skip in taps:
                term = tapf[tap : tap + 1] * piece[skip : skip + LANES]
                acc = term if acc is None else acc + term
        here = pl.ds(pl.multiple_of(at, LANES), LANES)
        sig = sigmoid(g_ref[0, here, :].astype(F32))
        v = v_ref[0, here, :].astype(F32)
        vg = acc * sig
        vg_ref[0, here, :] = vg.astype(BF16)
        gg_ref[0, here, :] = (vg * v * (1.0 - sig)).astype(BF16)
        return carry

    lax.fori_loop(0, blocks, block, 0, unroll=4)


def final_kernel(got_ref, w_ref, taps_ref, gain_ref, bias_ref):
    acc = got_ref[0].astype(F32)
    for p in range(1, got_ref.shape[0]):
        acc = acc + got_ref[p].astype(F32)
    width = w_ref.shape[1]
    w_ref[...] = acc[:, :width]
    for t in range(K // 8 + 1):
        tile = acc[:, width + t * LANES : width + (t + 1) * LANES]
        taps_ref[8 * t : min(8 * t + 8, K)] = tile[: min(8, K - 8 * t)]
    for ref, row in ((gain_ref, K), (bias_ref, K + 1)):
        at = width + row // 8 * LANES
        ref[...] = acc[row % 8 : row % 8 + 1, at : at + LANES]


def whole(shape):
    return pl.BlockSpec(shape, lambda i: (0,) * len(shape))


PARAMS = pltpu.CompilerParams(vmem_limit_bytes=67_043_328)


def cost(flops, moved):
    return pl.CostEstimate(flops=flops, bytes_accessed=moved, transcendentals=0)


def on_device(values_in, gates_in, conv_taps, conv_bias, norm_gain, out_weight, out_grad):
    seqs, length, chans = values_in.shape
    width = out_grad.shape[2]
    tokens = seqs * length
    blocks = length // LANES
    tp, sp = lax.axis_size("tp"), lax.axis_size("sp")
    stat_rows = 2 * tokens // LANES
    flat = out_grad.reshape(tokens, width)
    ahead = [(i, i + 1) for i in range(sp - 1)]
    back = [(i + 1, i) for i in range(sp - 1)]
    swap = [(i, i ^ 1) for i in range(tp)]
    core = (lax.axis_index("tp") % 2).astype(jnp.int32).reshape(1)
    bias_row = conv_bias.reshape(1, chans)
    gain_row = norm_gain.reshape(1, chans)

    SDS = jax.ShapeDtypeStruct
    any_ = pl.BlockSpec(memory_space=pl.ANY)
    vmem = pl.BlockSpec(memory_space=pltpu.VMEM)
    smem = pl.BlockSpec(memory_space=pltpu.SMEM)
    seq_block = pl.BlockSpec((1, length, chans), lambda i: (i, 0, 0))
    head_block = pl.BlockSpec((1, PAD, chans), lambda i: (i, 0, 0))
    gated_block = pl.BlockSpec((1, length + PAD, chans), lambda i: (i, 0, 0))
    col = pl.BlockSpec((chans, length), lambda i: (0, i))
    quarter = pl.BlockSpec((chans, length // 4), lambda i: (0, i))
    stats = whole((tp, stat_rows, LANES))

    tail = slice(length - PAD, length)
    edge = values_in[:, tail].astype(F32) * sigmoid(gates_in[:, tail].astype(F32))
    halo = lax.ppermute(edge.astype(BF16), "sp", ahead)
    weight2 = lax.ppermute(out_weight, "tp", swap)
    conv, pay, gated, mine_a, other_a = pl.pallas_call(
        functools.partial(conv_kernel, blocks),
        grid=(seqs,),
        in_specs=[
            smem,
            seq_block,
            seq_block,
            head_block,
            whole((K, chans)),
            whole((1, chans)),
            any_,
            any_,
            any_,
        ],
        out_specs=[col, stats, gated_block, quarter, quarter],
        out_shape=[
            SDS((chans, tokens), F32),
            SDS((tp, stat_rows, LANES), F32),
            SDS((seqs, length + PAD, chans), BF16),
            SDS((chans, tokens // 4), F32),
            SDS((chans, tokens // 4), BF16),
        ],
        scratch_shapes=[
            pltpu.VMEM((length + 2 * PAD, chans), F32),
            pltpu.VMEM((PAD, chans), F32),
            pltpu.VMEM((stat_rows, LANES), F32),
            pltpu.VMEM((2 * chans, width), BF16),
            pltpu.VMEM((seqs, length // 4, width), BF16),
            pltpu.SemaphoreType.DMA((2,)),
            pltpu.SemaphoreType.DMA((seqs,)),
        ],
        compiler_params=PARAMS,
        cost_estimate=cost(2 * K * tokens * chans, 8 << 20),
        name="conv",
    )(core, values_in, gates_in, halo, conv_taps, bias_row, out_weight, weight2, flat)
    got = lax.all_to_all(pay, "tp", 0, 0, tiled=True)

    pieces = 4
    half = seqs // 2
    other_a = lax.ppermute(other_a, "tp", swap)
    mine_b, other_b = pl.pallas_call(
        swish_kernel,
        in_specs=[smem, any_, any_, any_, any_],
        out_specs=[any_, any_],
        out_shape=[SDS((chans, tokens // 4), F32), SDS((chans, tokens // 4), BF16)],
        scratch_shapes=[
            pltpu.VMEM((2 * chans, width), BF16),
            pltpu.VMEM((half, length // 2, width), BF16),
            pltpu.VMEM((chans, tokens // 4), F32),
            pltpu.VMEM((chans, tokens // 4), BF16),
            pltpu.SemaphoreType.DMA((2,)),
            pltpu.SemaphoreType.DMA((half,)),
            pltpu.SemaphoreType.DMA((2 * half,)),
        ],
        compiler_params=PARAMS,
        cost_estimate=cost(tokens * chans * width, tokens * width // 2),
        name="swish_grad",
    )(core, out_weight, weight2, flat, pay)
    other_b = lax.ppermute(other_b, "tp", swap)

    turned = pl.BlockSpec((chans, length), lambda i, c: (0, (i + c[0] * half) % seqs))
    near = pl.BlockSpec((chans, length // 2), lambda i, c: (0, jnp.minimum(i, half - 1)))
    far = pl.BlockSpec((chans, length // 2), lambda i, c: (0, jnp.maximum(i, half) - half))
    swished, ng, pay2, stat, gg = pl.pallas_call(
        norm_kernel,
        grid_spec=pltpu.PrefetchScalarGridSpec(
            num_scalar_prefetch=1,
            grid=(seqs,),
            in_specs=[
                turned,
                near,
                far,
                near,
                far,
                pl.BlockSpec((tp, stat_rows, LANES), lambda i, c: (0, 0, 0)),
                pl.BlockSpec((1, chans), lambda i, c: (0, 0)),
            ],
            out_specs=[
                turned,
                turned,
                pl.BlockSpec((tp, stat_rows, LANES), lambda i, c: (0, 0, 0)),
                pl.BlockSpec((stat_rows, LANES), lambda i, c: (0, 0)),
                pl.BlockSpec((1, chans), lambda i, c: (0, 0)),
            ],
            scratch_shapes=[
                pltpu.VMEM((chans, LANES), F32),
                pltpu.VMEM((chans, LANES), F32),
                pltpu.VMEM((stat_rows, LANES), F32),
            ],
        ),
        out_shape=[
            SDS((chans, tokens), BF16),
            SDS((chans, tokens), F32),
            SDS((tp, stat_rows, LANES), F32),
            SDS((stat_rows, LANES), F32),
            SDS((1, chans), F32),
        ],
        compiler_params=PARAMS,
        cost_estimate=cost(30 * tokens * chans, 8 << 20),
        name="norm",
    )(core, conv, mine_a, other_a, mine_b, other_b, got, gain_row)
    got2 = lax.all_to_all(pay2, "tp", 0, 0, tiled=True)

    extra = -(-(K + 2) // 8) * LANES
    rows = chans // sp
    pieces = seqs
    cols = width // 2 // pieces
    slabs = [
        pltpu.VMEM((pieces, tokens, cols), BF16),
        pltpu.VMEM((pieces, sp, rows, cols), BF16),
    ]
    pay3 = pl.pallas_call(
        weight_kernel,
        in_specs=[vmem, any_],
        out_specs=any_,
        out_shape=SDS((sp, rows, width + extra), BF16),
        scratch_shapes=[
            *slabs,
            pltpu.SemaphoreType.DMA((pieces,)),
            pltpu.SemaphoreType.DMA((pieces,)),
        ],
        compiler_params=PARAMS,
        cost_estimate=cost(tokens * chans * width, tokens * width),
        name="weight_grad",
    )(swished, flat)

    cg, head, pay3 = pl.pallas_call(
        functools.partial(grad_kernel, blocks),
        grid=(seqs,),
        in_specs=[
            col,
            col,
            whole((stat_rows, LANES)),
            stats,
            gated_block,
            whole((1, chans)),
            vmem,
            any_,
            any_,
        ],
        out_specs=[seq_block, head_block, any_],
        out_shape=[
            SDS((seqs, length, chans), F32),
            SDS((seqs, PAD, chans), F32),
            SDS(pay3.shape, BF16),
        ],
        scratch_shapes=[
            pltpu.VMEM((length + PAD, chans), F32),
            pltpu.VMEM((K, 8, chans), F32),
            pltpu.VMEM((8, chans), F32),
            pltpu.VMEM((stat_rows, LANES), F32),
            pltpu.VMEM((sp, rows, extra), BF16),
            *slabs,
            pltpu.SemaphoreType.DMA,
            pltpu.SemaphoreType.DMA((pieces,)),
            pltpu.SemaphoreType.DMA((pieces,)),
        ],
        input_output_aliases={8: 2},
        compiler_params=PARAMS,
        cost_estimate=cost(2 * K * tokens * chans, 8 << 20),
        name="taps_grad",
    )(conv, ng, stat, got2, gated, gg, swished, flat, pay3)
    after = lax.ppermute(head, "sp", back)
    got3 = lax.all_to_all(pay3, "sp", 0, 0, tiled=True)

    values_grad, gates_grad = pl.pallas_call(
        functools.partial(spread_kernel, blocks),
        grid=(seqs,),
        in_specs=[seq_block, head_block, seq_block, seq_block, whole((K, chans))],
        out_specs=[seq_block, seq_block],
        out_shape=[SDS((seqs, length, chans), BF16)] * 2,
        scratch_shapes=[pltpu.VMEM((length + 2 * PAD, chans), F32), pltpu.VMEM((PAD, chans), F32)],
        compiler_params=PARAMS,
        cost_estimate=cost(2 * K * tokens * chans, 8 << 20),
        name="gated_grad",
    )(cg, after, values_in, gates_in, conv_taps)

    weight_grad, taps_grad, gain_grad, bias_grad = pl.pallas_call(
        final_kernel,
        in_specs=[vmem],
        out_specs=[vmem] * 4,
        out_shape=[
            SDS((chans // sp, width), F32),
            SDS((K, chans), F32),
            SDS((1, chans), F32),
            SDS((1, chans), F32),
        ],
        compiler_params=PARAMS,
        name="final_sum",
    )(got3)
    gain_grad, bias_grad = gain_grad.reshape(chans), bias_grad.reshape(chans)
    return values_grad, gates_grad, taps_grad, gain_grad, bias_grad, weight_grad


def solution(mesh):
    return jax.shard_map(
        on_device,
        mesh=mesh,
        in_specs=(
            P(None, "sp", "tp"),
            P(None, "sp", "tp"),
            P(None, "tp"),
            P("tp"),
            P("tp"),
            P("tp", None),
            P(None, "sp", None),
        ),
        out_specs=(
            P(None, "sp", "tp"),
            P(None, "sp", "tp"),
            P(None, "tp"),
            P("tp"),
            P("tp"),
            P(("tp", "sp"), None),
        ),
        check_vma=False,
    )
```

```python
import functools

import jax
import jax.numpy as jnp
from jax import lax
from jax.experimental import pallas as pl
from jax.experimental.pallas import tpu as pltpu
from jax.sharding import PartitionSpec as P


K = 31
REACH = K - 1
PAD = 32
EPS = 1e-05
LANES = 128
F32 = jnp.float32
BF16 = jnp.bfloat16


def sigmoid(x):
    return 0.5 * jnp.tanh(0.5 * x) + 0.5


def taps_by_shift(first):
    groups = {}
    for tap in range(K):
        groups.setdefault(first(tap) % 8, []).append((tap, first(tap) // 8 * 8))
    return sorted(groups.items())


def conv_kernel(
    blocks, core_ref, v_ref, g_ref, halo_ref, taps_ref, bias_ref, w_hbm, w2_hbm, og_hbm,
    conv_ref, pay_ref, gated_ref, mine_ref, other_ref,
    wide, tapf, rows, lhs, og, prod, wsem, sems,
):
    seq = pl.program_id(0)
    n, tok, _ = og.shape
    chans = mine_ref.shape[0]
    base = core_ref[0] * (og_hbm.shape[0] // 2)

    def fetch(i):
        at = base + i // 2 * (blocks * LANES) + i % 2 * tok
        return pltpu.make_async_copy(
            og_hbm.at[pl.ds(pl.multiple_of(at, tok), tok)], og.at[i], sems.at[i]
        )

    weights = [
        pltpu.make_async_copy(w_hbm, lhs.at[pl.ds(0, chans)], wsem.at[0]),
        pltpu.make_async_copy(w2_hbm, lhs.at[pl.ds(chans, chans)], wsem.at[1]),
    ]

    @pl.when(seq == 0)
    def _():
        for c in weights:
            c.start()
        fetch(0).start()
        tapf[:K] = taps_ref[...].astype(F32)

    @pl.when(seq < n - 1)
    def _():
        fetch(seq + 1).start()

    gated_ref[0, :PAD] = halo_ref[0]
    wide[:PAD] = halo_ref[0].astype(F32)
    for b in range(blocks):
        at = b * LANES
        y = v_ref[0, at : at + LANES].astype(F32) * sigmoid(g_ref[0, at : at + LANES].astype(F32))
        y = y.astype(BF16)
        gated_ref[0, PAD + at : PAD + at + LANES] = y
        wide[PAD + at : PAD + at + LANES] = y.astype(F32)
    bias = bias_ref[...].astype(F32)

    def block(b, carry):
        at = b * LANES
        acc = jnp.broadcast_to(bias, (LANES, LANES))
        for shift, taps in taps_by_shift(lambda tap: tap + PAD - REACH):
            piece = wide[pl.ds(at + shift, LANES + taps[-1][1]), :]
            for tap, skip in taps:
                acc = acc + tapf[tap : tap + 1] * piece[skip : skip + LANES]
        turned = acc.T
        conv_ref[:, pl.ds(pl.multiple_of(at, LANES), LANES)] = turned
        mean = jnp.sum(turned, axis=0, keepdims=True) * (1.0 / LANES)
        off = turned - mean
        row = seq * blocks + b
        rows[pl.ds(row, 1)] = mean
        rows[pl.ds(row + rows.shape[0] // 2, 1)] = jnp.sum(off * off, axis=0, keepdims=True)
        return carry

    lax.fori_loop(0, blocks // 2, block, 0, unroll=4)

    @pl.when(seq == 0)
    def _():
        for c in weights:
            c.wait()

    fetch(seq).wait()
    step = lhs.shape[1] // (blocks // 2)
    for j in range(blocks // 2):
        k = slice(j * step, (j + 1) * step)
        part = lax.dot_general(
            lhs[:, k], og[seq, :, k], (((1,), (1,)), ((), ())), preferred_element_type=F32
        )
        block(blocks // 2 + j, 0)
        prod[...] = part if j == 0 else prod[...] + part
    mine_ref[...] = prod[:chans]
    other_ref[...] = prod[chans:].astype(BF16)

    @pl.when(seq == pl.num_programs(0) - 1)
    def _():
        for peer in range(pay_ref.shape[0]):
            pay_ref[peer] = rows[...]


def swish_kernel(
    core_ref, w_hbm, w2_hbm, og_hbm, after_ref, mine_hbm, other_hbm,
    lhs, og, mine, other, wsem, sems, osems,
):
    n, tok, _ = og.shape
    chans = mine.shape[0]
    base = core_ref[0] * (2 * n * tok)
    ins = []
    for i in range(n):
        at = pl.multiple_of(base + (2 * i + 1) * tok, tok)
        ins.append(pltpu.make_async_copy(og_hbm.at[pl.ds(at, tok)], og.at[i], sems.at[i]))
    weights = [
        pltpu.make_async_copy(w_hbm, lhs.at[pl.ds(0, chans)], wsem.at[0]),
        pltpu.make_async_copy(w2_hbm, lhs.at[pl.ds(chans, chans)], wsem.at[1]),
    ]
    for c in weights + ins:
        c.start()
    for c in weights:
        c.wait()
    outs = []
    for i in range(n):
        ins[i].wait()
        here = pl.ds(i * tok, tok)
        out = lax.dot_general(
            lhs[...], og[i], (((1,), (1,)), ((), ())), preferred_element_type=F32
        )
        mine[:, here] = out[:chans]
        other[:, here] = out[chans:].astype(BF16)
        outs += [
            pltpu.make_async_copy(mine.at[:, here], mine_hbm.at[:, here], osems.at[2 * i]),
            pltpu.make_async_copy(other.at[:, here], other_hbm.at[:, here], osems.at[2 * i + 1]),
        ]
        for c in outs[-2:]:
            c.start()
    for c in outs:
        c.wait()


def norm_kernel(
    core_ref, conv_ref, mine_a, other_a, mine_b, other_b, got_ref, gain_ref,
    sw_ref, ng_ref, pay_ref, stat_ref, gg_ref, gcol, gacc, rows,
):
    step = pl.program_id(0)
    half = rows.shape[0] // 2
    peers = got_ref.shape[0]

    @pl.when(step == 0)
    def _():
        gain = jnp.broadcast_to(gain_ref[...].astype(F32), (LANES, LANES))
        gcol[...] = gain.T
        gacc[...] = jnp.zeros_like(gacc)
        mean = got_ref[0, :half]
        m2 = got_ref[0, half:]
        for p in range(1, peers):
            mean = mean + got_ref[p, :half]
            m2 = m2 + got_ref[p, half:]
        mean = mean * (1.0 / peers)
        apart = jnp.square(got_ref[0, :half] - mean)
        for p in range(1, peers):
            apart = apart + jnp.square(got_ref[p, :half] - mean)
        var = (m2 + LANES * apart) * (1.0 / (peers * LANES))
        stat_ref[:half] = mean
        stat_ref[half:] = lax.rsqrt(var + EPS)

    chunk = 32
    steps = pl.num_programs(0)
    seq = lax.rem(step + core_ref[0] * (steps // 2), steps)
    is_mine = step < steps // 2
    for j in range(conv_ref.shape[1] // LANES):
        at = j * LANES
        row = seq * (conv_ref.shape[1] // LANES) + j
        late = at >= mine_a.shape[1]
        mine_ref, other_ref = (mine_b, other_b) if late else (mine_a, other_a)
        near = at - mine_a.shape[1] if late else at
        mean = stat_ref[pl.ds(row, 1)]
        inverse = stat_ref[pl.ds(half + row, 1)]
        s1 = jnp.zeros((8, LANES), F32)
        s2 = jnp.zeros((8, LANES), F32)
        for c in range(0, LANES, chunk):
            normed = (conv_ref[c : c + chunk, at : at + LANES] - mean) * inverse
            gain = gcol[c : c + chunk]
            scaled = normed * gain
            sig = sigmoid(scaled)
            sw_ref[c : c + chunk, at : at + LANES] = (scaled * sig).astype(BF16)
            swg = jnp.where(
                is_mine,
                mine_ref[c : c + chunk, near : near + LANES],
                other_ref[c : c + chunk, near : near + LANES].astype(F32),
            )
            sg = swg * sig * (1.0 + scaled * (1.0 - sig))
            gacc[c : c + chunk] += sg * normed
            ng = sg * gain
            ng_ref[c : c + chunk, at : at + LANES] = ng
            nn = ng * normed
            for r in range(0, chunk, 8):
                s1 = s1 + ng[r : r + 8]
                s2 = s2 + nn[r : r + 8]
        rows[pl.ds(row, 1)] = jnp.sum(s1, axis=0, keepdims=True)
        rows[pl.ds(half + row, 1)] = jnp.sum(s2, axis=0, keepdims=True)

    @pl.when(step == pl.num_programs(0) - 1)
    def _():
        gg_ref[...] = jnp.sum(gacc[...].T, axis=0, keepdims=True)
        for peer in range(peers):
            pay_ref[peer] = rows[...]


def weight_kernel(sw_ref, og_hbm, out_hbm, og, out, sems, osems):
    n, _, cols = og.shape
    ins = [
        pltpu.make_async_copy(og_hbm.at[:, pl.ds(i * cols, cols)], og.at[i], sems.at[i])
        for i in range(n)
    ]
    outs = [
        pltpu.make_async_copy(out.at[i], out_hbm.at[:, :, pl.ds(i * cols, cols)], osems.at[i])
        for i in range(n)
    ]
    for c in ins:
        c.start()
    for i in range(n):
        ins[i].wait()
        part = jnp.dot(sw_ref[...], og[i], preferred_element_type=F32)
        out[i] = part.astype(BF16).reshape(out.shape[1:])
        outs[i].start()
    for c in outs:
        c.wait()


def grad_kernel(
    blocks, conv_ref, ng_ref, stat_ref, got_ref, gated_ref, gg_ref, sw_ref, og_hbm, pay_in,
    cg_ref, head_ref, pay_ref,
    wide, taps_acc, bias_acc, means, small, og, out, sem, sems, osems,
):
    seq = pl.program_id(0)
    n, _, cols = og.shape

    def fetch(i):
        at = pl.multiple_of((n + i) * cols, LANES)
        return pltpu.make_async_copy(og_hbm.at[:, pl.ds(at, cols)], og.at[i], sems.at[i])

    def send(i):
        at = pl.multiple_of((n + i) * cols, LANES)
        return pltpu.make_async_copy(out.at[i], pay_ref.at[:, :, pl.ds(at, cols)], osems.at[i])

    @pl.when(seq == 0)
    def _():
        fetch(0).start()

    @pl.when(seq < n - 1)
    def _():
        fetch(seq + 1).start()

    half = stat_ref.shape[0] // 2
    peers = got_ref.shape[0]
    total = peers * LANES

    @pl.when(seq == 0)
    def _():
        s = got_ref[0]
        for p in range(1, peers):
            s = s + got_ref[p]
        means[...] = s * (1.0 / total)
        bias_acc[...] = jnp.zeros_like(bias_acc)
        taps_acc[...] = jnp.zeros_like(taps_acc)

    wide[...] = gated_ref[0].astype(F32)

    def block(b, carry):
        at = b * LANES
        here = pl.ds(pl.multiple_of(at, LANES), LANES)
        row = seq * blocks + b
        mean = stat_ref[pl.ds(row, 1)]
        inverse = stat_ref[pl.ds(half + row, 1)]
        m1 = means[pl.ds(row, 1)]
        m2 = means[pl.ds(half + row, 1)]
        normed = (conv_ref[:, here] - mean) * inverse
        cg = inverse * (ng_ref[:, here] - m1 - normed * m2)
        cg = cg.T
        cg_ref[0, here, :] = cg
        part = cg[:8]
        for r in range(8, LANES, 8):
            part = part + cg[r : r + 8]
        bias_acc[...] += part
        for shift, taps in taps_by_shift(lambda tap: tap + PAD - REACH):
            piece = wide[pl.ds(at + shift, LANES + taps[-1][1]), :]
            for tap, skip in taps:
                acc = taps_acc[tap]
                for r in range(0, LANES, 8):
                    acc = acc + cg[r : r + 8] * piece[skip + r : skip + r + 8]
                taps_acc[tap] = acc
        return carry

    lax.fori_loop(0, blocks // 2, block, 0, unroll=2)
    fetch(seq).wait()
    out[seq] = (
        jnp.dot(sw_ref[...], og[seq], preferred_element_type=F32)
        .astype(BF16)
        .reshape(out.shape[1:])
    )
    for b in range(blocks // 2, blocks // 2 + 2):
        block(b, 0)
    lax.fori_loop(blocks // 2 + 2, blocks, block, 0, unroll=2)
    send(seq).start()
    head_ref[0] = cg_ref[0, :PAD]

    @pl.when(seq == pl.num_programs(0) - 1)
    def _():
        rows = [jnp.sum(taps_acc[tap], axis=0, keepdims=True) for tap in range(K)]
        rows += [gg_ref[...], jnp.sum(bias_acc[...], axis=0, keepdims=True)]
        rows += [jnp.zeros((1, LANES), F32)] * (-len(rows) % 8)
        for t in range(len(rows) // 8):
            tile = jnp.concatenate(rows[8 * t : 8 * t + 8], axis=0).astype(BF16)
            for peer in range(small.shape[0]):
                small[peer, :, t * LANES : (t + 1) * LANES] = tile
        copy = pltpu.make_async_copy(
            small, pay_ref.at[:, :, pl.ds(2 * n * cols, small.shape[2])], sem
        )
        copy.start()
        copy.wait()
        for i in range(n):
            send(i).wait()


def spread_kernel(blocks, cg_ref, next_ref, v_ref, g_ref, taps_ref, vg_ref, gg_ref, wide, tapf):
    @pl.when(pl.program_id(0) == 0)
    def _():
        tapf[:K] = taps_ref[...].astype(F32)

    length = blocks * LANES
    wide[:length] = cg_ref[0]
    wide[length : length + PAD] = next_ref[0]

    def block(b, carry):
        at = b * LANES
        acc = None
        for shift, taps in taps_by_shift(lambda tap: REACH - tap):
            piece = wide[pl.ds(at + shift, LANES + max(skip for _, skip in taps)), :]
            for tap, skip in taps:
                term = tapf[tap : tap + 1] * piece[skip : skip + LANES]
                acc = term if acc is None else acc + term
        here = pl.ds(pl.multiple_of(at, LANES), LANES)
        sig = sigmoid(g_ref[0, here, :].astype(F32))
        v = v_ref[0, here, :].astype(F32)
        vg = acc * sig
        vg_ref[0, here, :] = vg.astype(BF16)
        gg_ref[0, here, :] = (vg * v * (1.0 - sig)).astype(BF16)
        return carry

    lax.fori_loop(0, blocks, block, 0, unroll=4)


def final_kernel(got_ref, w_ref, taps_ref, gain_ref, bias_ref):
    acc = got_ref[0].astype(F32)
    for p in range(1, got_ref.shape[0]):
        acc = acc + got_ref[p].astype(F32)
    width = w_ref.shape[1]
    w_ref[...] = acc[:, :width]
    for t in range(K // 8 + 1):
        tile = acc[:, width + t * LANES : width + (t + 1) * LANES]
        taps_ref[8 * t : min(8 * t + 8, K)] = tile[: min(8, K - 8 * t)]
    for ref, row in ((gain_ref, K), (bias_ref, K + 1)):
        at = width + row // 8 * LANES
        ref[...] = acc[row % 8 : row % 8 + 1, at : at + LANES]


def whole(shape):
    return pl.BlockSpec(shape, lambda i: (0,) * len(shape))


PARAMS = pltpu.CompilerParams(vmem_limit_bytes=67_043_328)


def cost(flops, moved):
    return pl.CostEstimate(flops=flops, bytes_accessed=moved, transcendentals=0)


def on_device(values_in, gates_in, conv_taps, conv_bias, norm_gain, out_weight, out_grad):
    seqs, length, chans = values_in.shape
    width = out_grad.shape[2]
    tokens = seqs * length
    blocks = length // LANES
    tp, sp = lax.axis_size("tp"), lax.axis_size("sp")
    stat_rows = 2 * tokens // LANES
    flat = out_grad.reshape(tokens, width)
    ahead = [(i, i + 1) for i in range(sp - 1)]
    back = [(i + 1, i) for i in range(sp - 1)]
    swap = [(i, i ^ 1) for i in range(tp)]
    core = (lax.axis_index("tp") % 2).astype(jnp.int32).reshape(1)
    bias_row = conv_bias.reshape(1, chans)
    gain_row = norm_gain.reshape(1, chans)

    SDS = jax.ShapeDtypeStruct
    any_ = pl.BlockSpec(memory_space=pl.ANY)
    vmem = pl.BlockSpec(memory_space=pltpu.VMEM)
    smem = pl.BlockSpec(memory_space=pltpu.SMEM)
    seq_block = pl.BlockSpec((1, length, chans), lambda i: (i, 0, 0))
    head_block = pl.BlockSpec((1, PAD, chans), lambda i: (i, 0, 0))
    gated_block = pl.BlockSpec((1, length + PAD, chans), lambda i: (i, 0, 0))
    col = pl.BlockSpec((chans, length), lambda i: (0, i))
    quarter = pl.BlockSpec((chans, length // 4), lambda i: (0, i))
    stats = whole((tp, stat_rows, LANES))

    tail = slice(length - PAD, length)
    edge = values_in[:, tail].astype(F32) * sigmoid(gates_in[:, tail].astype(F32))
    halo = lax.ppermute(edge.astype(BF16), "sp", ahead)
    weight2 = lax.ppermute(out_weight, "tp", swap)
    conv, pay, gated, mine_a, other_a = pl.pallas_call(
        functools.partial(conv_kernel, blocks),
        grid=(seqs,),
        in_specs=[
            smem,
            seq_block,
            seq_block,
            head_block,
            whole((K, chans)),
            whole((1, chans)),
            any_,
            any_,
            any_,
        ],
        out_specs=[col, stats, gated_block, quarter, quarter],
        out_shape=[
            SDS((chans, tokens), F32),
            SDS((tp, stat_rows, LANES), F32),
            SDS((seqs, length + PAD, chans), BF16),
            SDS((chans, tokens // 4), F32),
            SDS((chans, tokens // 4), BF16),
        ],
        scratch_shapes=[
            pltpu.VMEM((length + 2 * PAD, chans), F32),
            pltpu.VMEM((PAD, chans), F32),
            pltpu.VMEM((stat_rows, LANES), F32),
            pltpu.VMEM((2 * chans, width), BF16),
            pltpu.VMEM((seqs, length // 4, width), BF16),
            pltpu.VMEM((2 * chans, length // 4), F32),
            pltpu.SemaphoreType.DMA((2,)),
            pltpu.SemaphoreType.DMA((seqs,)),
        ],
        compiler_params=PARAMS,
        cost_estimate=cost(2 * K * tokens * chans, 8 << 20),
        name="conv",
    )(core, values_in, gates_in, halo, conv_taps, bias_row, out_weight, weight2, flat)
    got = lax.all_to_all(pay, "tp", 0, 0, tiled=True)

    pieces = 4
    half = seqs // 2
    other_a = lax.ppermute(other_a, "tp", swap)
    mine_b, other_b = pl.pallas_call(
        swish_kernel,
        in_specs=[smem, any_, any_, any_, any_],
        out_specs=[any_, any_],
        out_shape=[SDS((chans, tokens // 4), F32), SDS((chans, tokens // 4), BF16)],
        scratch_shapes=[
            pltpu.VMEM((2 * chans, width), BF16),
            pltpu.VMEM((half, length // 2, width), BF16),
            pltpu.VMEM((chans, tokens // 4), F32),
            pltpu.VMEM((chans, tokens // 4), BF16),
            pltpu.SemaphoreType.DMA((2,)),
            pltpu.SemaphoreType.DMA((half,)),
            pltpu.SemaphoreType.DMA((2 * half,)),
        ],
        compiler_params=PARAMS,
        cost_estimate=cost(tokens * chans * width, tokens * width // 2),
        name="swish_grad",
    )(core, out_weight, weight2, flat, pay)
    other_b = lax.ppermute(other_b, "tp", swap)

    turned = pl.BlockSpec((chans, length), lambda i, c: (0, (i + c[0] * half) % seqs))
    near = pl.BlockSpec((chans, length // 2), lambda i, c: (0, jnp.minimum(i, half - 1)))
    far = pl.BlockSpec((chans, length // 2), lambda i, c: (0, jnp.maximum(i, half) - half))
    swished, ng, pay2, stat, gg = pl.pallas_call(
        norm_kernel,
        grid_spec=pltpu.PrefetchScalarGridSpec(
            num_scalar_prefetch=1,
            grid=(seqs,),
            in_specs=[
                turned,
                near,
                far,
                near,
                far,
                pl.BlockSpec((tp, stat_rows, LANES), lambda i, c: (0, 0, 0)),
                pl.BlockSpec((1, chans), lambda i, c: (0, 0)),
            ],
            out_specs=[
                turned,
                turned,
                pl.BlockSpec((tp, stat_rows, LANES), lambda i, c: (0, 0, 0)),
                pl.BlockSpec((stat_rows, LANES), lambda i, c: (0, 0)),
                pl.BlockSpec((1, chans), lambda i, c: (0, 0)),
            ],
            scratch_shapes=[
                pltpu.VMEM((chans, LANES), F32),
                pltpu.VMEM((chans, LANES), F32),
                pltpu.VMEM((stat_rows, LANES), F32),
            ],
        ),
        out_shape=[
            SDS((chans, tokens), BF16),
            SDS((chans, tokens), F32),
            SDS((tp, stat_rows, LANES), F32),
            SDS((stat_rows, LANES), F32),
            SDS((1, chans), F32),
        ],
        compiler_params=PARAMS,
        cost_estimate=cost(30 * tokens * chans, 8 << 20),
        name="norm",
    )(core, conv, mine_a, other_a, mine_b, other_b, got, gain_row)
    got2 = lax.all_to_all(pay2, "tp", 0, 0, tiled=True)

    extra = -(-(K + 2) // 8) * LANES
    rows = chans // sp
    pieces = seqs
    cols = width // 2 // pieces
    slabs = [
        pltpu.VMEM((pieces, tokens, cols), BF16),
        pltpu.VMEM((pieces, sp, rows, cols), BF16),
    ]
    pay3 = pl.pallas_call(
        weight_kernel,
        in_specs=[vmem, any_],
        out_specs=any_,
        out_shape=SDS((sp, rows, width + extra), BF16),
        scratch_shapes=[
            *slabs,
            pltpu.SemaphoreType.DMA((pieces,)),
            pltpu.SemaphoreType.DMA((pieces,)),
        ],
        compiler_params=PARAMS,
        cost_estimate=cost(tokens * chans * width, tokens * width),
        name="weight_grad",
    )(swished, flat)

    cg, head, pay3 = pl.pallas_call(
        functools.partial(grad_kernel, blocks),
        grid=(seqs,),
        in_specs=[
            col,
            col,
            whole((stat_rows, LANES)),
            stats,
            gated_block,
            whole((1, chans)),
            vmem,
            any_,
            any_,
        ],
        out_specs=[seq_block, head_block, any_],
        out_shape=[
            SDS((seqs, length, chans), F32),
            SDS((seqs, PAD, chans), F32),
            SDS(pay3.shape, BF16),
        ],
        scratch_shapes=[
            pltpu.VMEM((length + PAD, chans), F32),
            pltpu.VMEM((K, 8, chans), F32),
            pltpu.VMEM((8, chans), F32),
            pltpu.VMEM((stat_rows, LANES), F32),
            pltpu.VMEM((sp, rows, extra), BF16),
            *slabs,
            pltpu.SemaphoreType.DMA,
            pltpu.SemaphoreType.DMA((pieces,)),
            pltpu.SemaphoreType.DMA((pieces,)),
        ],
        input_output_aliases={8: 2},
        compiler_params=PARAMS,
        cost_estimate=cost(2 * K * tokens * chans, 8 << 20),
        name="taps_grad",
    )(conv, ng, stat, got2, gated, gg, swished, flat, pay3)
    after = lax.ppermute(head, "sp", back)
    got3 = lax.all_to_all(pay3, "sp", 0, 0, tiled=True)

    values_grad, gates_grad = pl.pallas_call(
        functools.partial(spread_kernel, blocks),
        grid=(seqs,),
        in_specs=[seq_block, head_block, seq_block, seq_block, whole((K, chans))],
        out_specs=[seq_block, seq_block],
        out_shape=[SDS((seqs, length, chans), BF16)] * 2,
        scratch_shapes=[pltpu.VMEM((length + 2 * PAD, chans), F32), pltpu.VMEM((PAD, chans), F32)],
        compiler_params=PARAMS,
        cost_estimate=cost(2 * K * tokens * chans, 8 << 20),
        name="gated_grad",
    )(cg, after, values_in, gates_in, conv_taps)

    weight_grad, taps_grad, gain_grad, bias_grad = pl.pallas_call(
        final_kernel,
        in_specs=[vmem],
        out_specs=[vmem] * 4,
        out_shape=[
            SDS((chans // sp, width), F32),
            SDS((K, chans), F32),
            SDS((1, chans), F32),
            SDS((1, chans), F32),
        ],
        compiler_params=PARAMS,
        name="final_sum",
    )(got3)
    gain_grad, bias_grad = gain_grad.reshape(chans), bias_grad.reshape(chans)
    return values_grad, gates_grad, taps_grad, gain_grad, bias_grad, weight_grad


def solution(mesh):
    return jax.shard_map(
        on_device,
        mesh=mesh,
        in_specs=(
            P(None, "sp", "tp"),
            P(None, "sp", "tp"),
            P(None, "tp"),
            P("tp"),
            P("tp"),
            P("tp", None),
            P(None, "sp", None),
        ),
        out_specs=(
            P(None, "sp", "tp"),
            P(None, "sp", "tp"),
            P(None, "tp"),
            P("tp"),
            P("tp"),
            P(("tp", "sp"), None),
        ),
        check_vma=False,
    )
```

```python
import functools

import jax
import jax.numpy as jnp
from jax import lax
from jax.experimental import pallas as pl
from jax.experimental.pallas import tpu as pltpu
from jax.sharding import PartitionSpec as P


K = 31
REACH = K - 1
PAD = 32
EPS = 1e-05
LANES = 128
F32 = jnp.float32
BF16 = jnp.bfloat16


def sigmoid(x):
    return 0.5 * jnp.tanh(0.5 * x) + 0.5


def taps_by_shift(first):
    groups = {}
    for tap in range(K):
        groups.setdefault(first(tap) % 8, []).append((tap, first(tap) // 8 * 8))
    return sorted(groups.items())


def conv_kernel(
    blocks, core_ref, v_ref, g_ref, halo_ref, taps_ref, bias_ref, w_hbm, w2_hbm, og_hbm,
    conv_ref, pay_ref, gated_ref, mine_ref, other_ref, wide, tapf, rows, lhs, og, wsem, sems,
):
    seq = pl.program_id(0)
    n, tok, _ = og.shape
    chans = mine_ref.shape[0]
    base = core_ref[0] * (og_hbm.shape[0] // 2)

    def fetch(i):
        at = base + i // 2 * (blocks * LANES) + i % 2 * tok
        return pltpu.make_async_copy(
            og_hbm.at[pl.ds(pl.multiple_of(at, tok), tok)], og.at[i], sems.at[i]
        )

    weights = [
        pltpu.make_async_copy(w_hbm, lhs.at[pl.ds(0, chans)], wsem.at[0]),
        pltpu.make_async_copy(w2_hbm, lhs.at[pl.ds(chans, chans)], wsem.at[1]),
    ]

    @pl.when(seq == 0)
    def _():
        for c in weights:
            c.start()
        fetch(0).start()
        tapf[:K] = taps_ref[...].astype(F32)

    gated_ref[0, :PAD] = halo_ref[0]
    wide[:PAD] = halo_ref[0].astype(F32)
    for b in range(blocks):
        at = b * LANES
        y = v_ref[0, at : at + LANES].astype(F32) * sigmoid(g_ref[0, at : at + LANES].astype(F32))
        y = y.astype(BF16)
        gated_ref[0, PAD + at : PAD + at + LANES] = y
        wide[PAD + at : PAD + at + LANES] = y.astype(F32)
    bias = bias_ref[...].astype(F32)

    def block(b, carry):
        at = b * LANES
        acc = jnp.broadcast_to(bias, (LANES, LANES))
        for shift, taps in taps_by_shift(lambda tap: tap + PAD - REACH):
            piece = wide[pl.ds(at + shift, LANES + taps[-1][1]), :]
            for tap, skip in taps:
                acc = acc + tapf[tap : tap + 1] * piece[skip : skip + LANES]
        turned = acc.T
        conv_ref[:, pl.ds(pl.multiple_of(at, LANES), LANES)] = turned
        mean = jnp.sum(turned, axis=0, keepdims=True) * (1.0 / LANES)
        off = turned - mean
        row = seq * blocks + b
        rows[pl.ds(row, 1)] = mean
        rows[pl.ds(row + rows.shape[0] // 2, 1)] = jnp.sum(off * off, axis=0, keepdims=True)
        return carry

    lax.fori_loop(0, blocks // 2, block, 0, unroll=4)

    @pl.when(seq == 0)
    def _():
        for c in weights:
            c.wait()

    fetch(seq).wait()

    @pl.when(seq < n - 1)
    def _():
        fetch(seq + 1).start()

    out = lax.dot_general(lhs[...], og[seq], (((1,), (1,)), ((), ())), preferred_element_type=F32)
    mine_ref[...] = out[:chans]
    other_ref[...] = out[chans:].astype(BF16)
    for b in range(blocks // 2, blocks):
        block(b, 0)

    @pl.when(seq == pl.num_programs(0) - 1)
    def _():
        for peer in range(pay_ref.shape[0]):
            pay_ref[peer] = rows[...]


def swish_kernel(
    core_ref, w_hbm, w2_hbm, og_hbm, after_ref, mine_hbm, other_hbm,
    lhs, og, mine, other, wsem, sems, osems,
):
    n, tok, _ = og.shape
    chans = mine.shape[0]
    base = core_ref[0] * (2 * n * tok)
    ins = []
    for i in range(n):
        at = pl.multiple_of(base + (2 * i + 1) * tok, tok)
        ins.append(pltpu.make_async_copy(og_hbm.at[pl.ds(at, tok)], og.at[i], sems.at[i]))
    weights = [
        pltpu.make_async_copy(w_hbm, lhs.at[pl.ds(0, chans)], wsem.at[0]),
        pltpu.make_async_copy(w2_hbm, lhs.at[pl.ds(chans, chans)], wsem.at[1]),
    ]
    for c in weights + ins:
        c.start()
    for c in weights:
        c.wait()
    outs = []
    for i in range(n):
        ins[i].wait()
        here = pl.ds(i * tok, tok)
        out = lax.dot_general(
            lhs[...], og[i], (((1,), (1,)), ((), ())), preferred_element_type=F32
        )
        mine[:, here] = out[:chans]
        other[:, here] = out[chans:].astype(BF16)
        outs += [
            pltpu.make_async_copy(mine.at[:, here], mine_hbm.at[:, here], osems.at[2 * i]),
            pltpu.make_async_copy(other.at[:, here], other_hbm.at[:, here], osems.at[2 * i + 1]),
        ]
        for c in outs[-2:]:
            c.start()
    for c in outs:
        c.wait()


def norm_kernel(
    core_ref, conv_ref, mine_a, other_a, mine_b, other_b, got_ref, gain_ref,
    sw_ref, ng_ref, pay_ref, stat_ref, gg_ref, gcol, gacc, rows,
):
    step = pl.program_id(0)
    half = rows.shape[0] // 2
    peers = got_ref.shape[0]

    @pl.when(step == 0)
    def _():
        gain = jnp.broadcast_to(gain_ref[...].astype(F32), (LANES, LANES))
        gcol[...] = gain.T
        gacc[...] = jnp.zeros_like(gacc)
        mean = got_ref[0, :half]
        m2 = got_ref[0, half:]
        for p in range(1, peers):
            mean = mean + got_ref[p, :half]
            m2 = m2 + got_ref[p, half:]
        mean = mean * (1.0 / peers)
        apart = jnp.square(got_ref[0, :half] - mean)
        for p in range(1, peers):
            apart = apart + jnp.square(got_ref[p, :half] - mean)
        var = (m2 + LANES * apart) * (1.0 / (peers * LANES))
        stat_ref[:half] = mean
        stat_ref[half:] = lax.rsqrt(var + EPS)

    chunk = 32
    steps = pl.num_programs(0)
    seq = lax.rem(step + core_ref[0] * (steps // 2), steps)
    is_mine = step < steps // 2
    for j in range(conv_ref.shape[1] // LANES):
        at = j * LANES
        row = seq * (conv_ref.shape[1] // LANES) + j
        late = at >= mine_a.shape[1]
        mine_ref, other_ref = (mine_b, other_b) if late else (mine_a, other_a)
        near = at - mine_a.shape[1] if late else at
        mean = stat_ref[pl.ds(row, 1)]
        inverse = stat_ref[pl.ds(half + row, 1)]
        s1 = jnp.zeros((8, LANES), F32)
        s2 = jnp.zeros((8, LANES), F32)
        for c in range(0, LANES, chunk):
            normed = (conv_ref[c : c + chunk, at : at + LANES] - mean) * inverse
            gain = gcol[c : c + chunk]
            scaled = normed * gain
            sig = sigmoid(scaled)
            sw_ref[c : c + chunk, at : at + LANES] = (scaled * sig).astype(BF16)
            swg = jnp.where(
                is_mine,
                mine_ref[c : c + chunk, near : near + LANES],
                other_ref[c : c + chunk, near : near + LANES].astype(F32),
            )
            sg = swg * sig * (1.0 + scaled * (1.0 - sig))
            gacc[c : c + chunk] += sg * normed
            ng = sg * gain
            ng_ref[c : c + chunk, at : at + LANES] = ng
            nn = ng * normed
            for r in range(0, chunk, 8):
                s1 = s1 + ng[r : r + 8]
                s2 = s2 + nn[r : r + 8]
        rows[pl.ds(row, 1)] = jnp.sum(s1, axis=0, keepdims=True)
        rows[pl.ds(half + row, 1)] = jnp.sum(s2, axis=0, keepdims=True)

    @pl.when(step == pl.num_programs(0) - 1)
    def _():
        gg_ref[...] = jnp.sum(gacc[...].T, axis=0, keepdims=True)
        for peer in range(peers):
            pay_ref[peer] = rows[...]


def weight_kernel(sw_ref, og_hbm, out_hbm, og, out, sems, osems):
    n, _, cols = og.shape
    ins = [
        pltpu.make_async_copy(og_hbm.at[:, pl.ds(i * cols, cols)], og.at[i], sems.at[i])
        for i in range(n)
    ]
    outs = [
        pltpu.make_async_copy(out.at[i], out_hbm.at[:, :, pl.ds(i * cols, cols)], osems.at[i])
        for i in range(n)
    ]
    for c in ins:
        c.start()
    for i in range(n):
        ins[i].wait()
        part = jnp.dot(sw_ref[...], og[i], preferred_element_type=F32)
        out[i] = part.astype(BF16).reshape(out.shape[1:])
        outs[i].start()
    for c in outs:
        c.wait()


def grad_kernel(
    blocks, conv_ref, ng_ref, stat_ref, got_ref, gated_ref, gg_ref, sw_hbm, og_hbm, pay_in,
    cg_ref, head_ref, pay_ref,
    wide, taps_acc, bias_acc, means, small, og, out, sw_ref, sem, sems, osems,
):
    seq = pl.program_id(0)
    n, _, cols = og.shape
    side = pltpu.make_async_copy(sw_hbm, sw_ref, sem)

    def fetch(i):
        at = pl.multiple_of((n + i) * cols, LANES)
        return pltpu.make_async_copy(og_hbm.at[:, pl.ds(at, cols)], og.at[i], sems.at[i])

    def send(i):
        at = pl.multiple_of((n + i) * cols, LANES)
        return pltpu.make_async_copy(out.at[i], pay_ref.at[:, :, pl.ds(at, cols)], osems.at[i])

    @pl.when(seq == 0)
    def _():
        side.start()
        fetch(0).start()

    half = stat_ref.shape[0] // 2
    peers = got_ref.shape[0]
    total = peers * LANES

    @pl.when(seq == 0)
    def _():
        s = got_ref[0]
        for p in range(1, peers):
            s = s + got_ref[p]
        means[...] = s * (1.0 / total)
        bias_acc[...] = jnp.zeros_like(bias_acc)
        taps_acc[...] = jnp.zeros_like(taps_acc)

    wide[...] = gated_ref[0].astype(F32)

    def block(b, carry):
        at = b * LANES
        here = pl.ds(pl.multiple_of(at, LANES), LANES)
        row = seq * blocks + b
        mean = stat_ref[pl.ds(row, 1)]
        inverse = stat_ref[pl.ds(half + row, 1)]
        m1 = means[pl.ds(row, 1)]
        m2 = means[pl.ds(half + row, 1)]
        normed = (conv_ref[:, here] - mean) * inverse
        cg = inverse * (ng_ref[:, here] - m1 - normed * m2)
        cg = cg.T
        cg_ref[0, here, :] = cg
        part = cg[:8]
        for r in range(8, LANES, 8):
            part = part + cg[r : r + 8]
        bias_acc[...] += part
        for shift, taps in taps_by_shift(lambda tap: tap + PAD - REACH):
            piece = wide[pl.ds(at + shift, LANES + taps[-1][1]), :]
            for tap, skip in taps:
                acc = taps_acc[tap]
                for r in range(0, LANES, 8):
                    acc = acc + cg[r : r + 8] * piece[skip + r : skip + r + 8]
                taps_acc[tap] = acc
        return carry

    lax.fori_loop(0, blocks // 2, block, 0, unroll=2)
    fetch(seq).wait()

    @pl.when(seq < n - 1)
    def _():
        fetch(seq + 1).start()

    @pl.when(seq == 0)
    def _():
        side.wait()

    out[seq] = (
        jnp.dot(sw_ref[...], og[seq], preferred_element_type=F32)
        .astype(BF16)
        .reshape(out.shape[1:])
    )
    for b in range(blocks // 2, blocks // 2 + 2):
        block(b, 0)
    lax.fori_loop(blocks // 2 + 2, blocks, block, 0, unroll=2)
    send(seq).start()
    head_ref[0] = cg_ref[0, :PAD]

    @pl.when(seq == pl.num_programs(0) - 1)
    def _():
        rows = [jnp.sum(taps_acc[tap], axis=0, keepdims=True) for tap in range(K)]
        rows += [gg_ref[...], jnp.sum(bias_acc[...], axis=0, keepdims=True)]
        rows += [jnp.zeros((1, LANES), F32)] * (-len(rows) % 8)
        for t in range(len(rows) // 8):
            tile = jnp.concatenate(rows[8 * t : 8 * t + 8], axis=0).astype(BF16)
            for peer in range(small.shape[0]):
                small[peer, :, t * LANES : (t + 1) * LANES] = tile
        copy = pltpu.make_async_copy(
            small, pay_ref.at[:, :, pl.ds(2 * n * cols, small.shape[2])], sem
        )
        copy.start()
        copy.wait()
        for i in range(n):
            send(i).wait()


def spread_kernel(blocks, cg_ref, next_ref, v_ref, g_ref, taps_ref, vg_ref, gg_ref, wide, tapf):
    @pl.when(pl.program_id(0) == 0)
    def _():
        tapf[:K] = taps_ref[...].astype(F32)

    length = blocks * LANES
    wide[:length] = cg_ref[0]
    wide[length : length + PAD] = next_ref[0]

    def block(b, carry):
        at = b * LANES
        acc = None
        for shift, taps in taps_by_shift(lambda tap: REACH - tap):
            piece = wide[pl.ds(at + shift, LANES + max(skip for _, skip in taps)), :]
            for tap, skip in taps:
                term = tapf[tap : tap + 1] * piece[skip : skip + LANES]
                acc = term if acc is None else acc + term
        here = pl.ds(pl.multiple_of(at, LANES), LANES)
        sig = sigmoid(g_ref[0, here, :].astype(F32))
        v = v_ref[0, here, :].astype(F32)
        vg = acc * sig
        vg_ref[0, here, :] = vg.astype(BF16)
        gg_ref[0, here, :] = (vg * v * (1.0 - sig)).astype(BF16)
        return carry

    lax.fori_loop(0, blocks, block, 0, unroll=4)


def final_kernel(got_ref, w_ref, taps_ref, gain_ref, bias_ref):
    acc = got_ref[0].astype(F32)
    for p in range(1, got_ref.shape[0]):
        acc = acc + got_ref[p].astype(F32)
    width = w_ref.shape[1]
    w_ref[...] = acc[:, :width]
    for t in range(K // 8 + 1):
        tile = acc[:, width + t * LANES : width + (t + 1) * LANES]
        taps_ref[8 * t : min(8 * t + 8, K)] = tile[: min(8, K - 8 * t)]
    for ref, row in ((gain_ref, K), (bias_ref, K + 1)):
        at = width + row // 8 * LANES
        ref[...] = acc[row % 8 : row % 8 + 1, at : at + LANES]


def whole(shape):
    return pl.BlockSpec(shape, lambda i: (0,) * len(shape))


PARAMS = pltpu.CompilerParams(vmem_limit_bytes=67_043_328)


def cost(flops, moved):
    return pl.CostEstimate(flops=flops, bytes_accessed=moved, transcendentals=0)


def on_device(values_in, gates_in, conv_taps, conv_bias, norm_gain, out_weight, out_grad):
    seqs, length, chans = values_in.shape
    width = out_grad.shape[2]
    tokens = seqs * length
    blocks = length // LANES
    tp, sp = lax.axis_size("tp"), lax.axis_size("sp")
    stat_rows = 2 * tokens // LANES
    flat = out_grad.reshape(tokens, width)
    ahead = [(i, i + 1) for i in range(sp - 1)]
    back = [(i + 1, i) for i in range(sp - 1)]
    swap = [(i, i ^ 1) for i in range(tp)]
    core = (lax.axis_index("tp") % 2).astype(jnp.int32).reshape(1)
    bias_row = conv_bias.reshape(1, chans)
    gain_row = norm_gain.reshape(1, chans)

    SDS = jax.ShapeDtypeStruct
    any_ = pl.BlockSpec(memory_space=pl.ANY)
    vmem = pl.BlockSpec(memory_space=pltpu.VMEM)
    smem = pl.BlockSpec(memory_space=pltpu.SMEM)
    seq_block = pl.BlockSpec((1, length, chans), lambda i: (i, 0, 0))
    head_block = pl.BlockSpec((1, PAD, chans), lambda i: (i, 0, 0))
    gated_block = pl.BlockSpec((1, length + PAD, chans), lambda i: (i, 0, 0))
    col = pl.BlockSpec((chans, length), lambda i: (0, i))
    quarter = pl.BlockSpec((chans, length // 4), lambda i: (0, i))
    stats = whole((tp, stat_rows, LANES))

    tail = slice(length - PAD, length)
    edge = values_in[:, tail].astype(F32) * sigmoid(gates_in[:, tail].astype(F32))
    halo = lax.ppermute(edge.astype(BF16), "sp", ahead)
    weight2 = lax.ppermute(out_weight, "tp", swap)
    conv, pay, gated, mine_a, other_a = pl.pallas_call(
        functools.partial(conv_kernel, blocks),
        grid=(seqs,),
        in_specs=[
            smem,
            seq_block,
            seq_block,
            head_block,
            whole((K, chans)),
            whole((1, chans)),
            any_,
            any_,
            any_,
        ],
        out_specs=[col, stats, gated_block, quarter, quarter],
        out_shape=[
            SDS((chans, tokens), F32),
            SDS((tp, stat_rows, LANES), F32),
            SDS((seqs, length + PAD, chans), BF16),
            SDS((chans, tokens // 4), F32),
            SDS((chans, tokens // 4), BF16),
        ],
        scratch_shapes=[
            pltpu.VMEM((length + 2 * PAD, chans), F32),
            pltpu.VMEM((PAD, chans), F32),
            pltpu.VMEM((stat_rows, LANES), F32),
            pltpu.VMEM((2 * chans, width), BF16),
            pltpu.VMEM((seqs, length // 4, width), BF16),
            pltpu.SemaphoreType.DMA((2,)),
            pltpu.SemaphoreType.DMA((seqs,)),
        ],
        compiler_params=PARAMS,
        cost_estimate=cost(2 * K * tokens * chans, 8 << 20),
        name="conv",
    )(core, values_in, gates_in, halo, conv_taps, bias_row, out_weight, weight2, flat)
    got = lax.all_to_all(pay, "tp", 0, 0, tiled=True)

    pieces = 4
    half = seqs // 2
    other_a = lax.ppermute(other_a, "tp", swap)
    mine_b, other_b = pl.pallas_call(
        swish_kernel,
        in_specs=[smem, any_, any_, any_, any_],
        out_specs=[any_, any_],
        out_shape=[SDS((chans, tokens // 4), F32), SDS((chans, tokens // 4), BF16)],
        scratch_shapes=[
            pltpu.VMEM((2 * chans, width), BF16),
            pltpu.VMEM((half, length // 2, width), BF16),
            pltpu.VMEM((chans, tokens // 4), F32),
            pltpu.VMEM((chans, tokens // 4), BF16),
            pltpu.SemaphoreType.DMA((2,)),
            pltpu.SemaphoreType.DMA((half,)),
            pltpu.SemaphoreType.DMA((2 * half,)),
        ],
        compiler_params=PARAMS,
        cost_estimate=cost(tokens * chans * width, tokens * width // 2),
        name="swish_grad",
    )(core, out_weight, weight2, flat, pay)
    other_b = lax.ppermute(other_b, "tp", swap)

    turned = pl.BlockSpec((chans, length), lambda i, c: (0, (i + c[0] * half) % seqs))
    near = pl.BlockSpec((chans, length // 2), lambda i, c: (0, jnp.minimum(i, half - 1)))
    far = pl.BlockSpec((chans, length // 2), lambda i, c: (0, jnp.maximum(i, half) - half))
    swished, ng, pay2, stat, gg = pl.pallas_call(
        norm_kernel,
        grid_spec=pltpu.PrefetchScalarGridSpec(
            num_scalar_prefetch=1,
            grid=(seqs,),
            in_specs=[
                turned,
                near,
                far,
                near,
                far,
                pl.BlockSpec((tp, stat_rows, LANES), lambda i, c: (0, 0, 0)),
                pl.BlockSpec((1, chans), lambda i, c: (0, 0)),
            ],
            out_specs=[
                turned,
                turned,
                pl.BlockSpec((tp, stat_rows, LANES), lambda i, c: (0, 0, 0)),
                pl.BlockSpec((stat_rows, LANES), lambda i, c: (0, 0)),
                pl.BlockSpec((1, chans), lambda i, c: (0, 0)),
            ],
            scratch_shapes=[
                pltpu.VMEM((chans, LANES), F32),
                pltpu.VMEM((chans, LANES), F32),
                pltpu.VMEM((stat_rows, LANES), F32),
            ],
        ),
        out_shape=[
            SDS((chans, tokens), BF16),
            SDS((chans, tokens), F32),
            SDS((tp, stat_rows, LANES), F32),
            SDS((stat_rows, LANES), F32),
            SDS((1, chans), F32),
        ],
        compiler_params=PARAMS,
        cost_estimate=cost(30 * tokens * chans, 8 << 20),
        name="norm",
    )(core, conv, mine_a, other_a, mine_b, other_b, got, gain_row)
    got2 = lax.all_to_all(pay2, "tp", 0, 0, tiled=True)

    extra = -(-(K + 2) // 8) * LANES
    rows = chans // sp
    pieces = seqs
    cols = width // 2 // pieces
    slabs = [
        pltpu.VMEM((pieces, tokens, cols), BF16),
        pltpu.VMEM((pieces, sp, rows, cols), BF16),
    ]
    pay3 = pl.pallas_call(
        weight_kernel,
        in_specs=[vmem, any_],
        out_specs=any_,
        out_shape=SDS((sp, rows, width + extra), BF16),
        scratch_shapes=[
            *slabs,
            pltpu.SemaphoreType.DMA((pieces,)),
            pltpu.SemaphoreType.DMA((pieces,)),
        ],
        compiler_params=PARAMS,
        cost_estimate=cost(tokens * chans * width, tokens * width),
        name="weight_grad",
    )(swished, flat)

    cg, head, pay3 = pl.pallas_call(
        functools.partial(grad_kernel, blocks),
        grid=(seqs,),
        in_specs=[
            col,
            col,
            whole((stat_rows, LANES)),
            stats,
            gated_block,
            whole((1, chans)),
            any_,
            any_,
            any_,
        ],
        out_specs=[seq_block, head_block, any_],
        out_shape=[
            SDS((seqs, length, chans), F32),
            SDS((seqs, PAD, chans), F32),
            SDS(pay3.shape, BF16),
        ],
        scratch_shapes=[
            pltpu.VMEM((length + PAD, chans), F32),
            pltpu.VMEM((K, 8, chans), F32),
            pltpu.VMEM((8, chans), F32),
            pltpu.VMEM((stat_rows, LANES), F32),
            pltpu.VMEM((sp, rows, extra), BF16),
            *slabs,
            pltpu.VMEM((chans, tokens), BF16),
            pltpu.SemaphoreType.DMA,
            pltpu.SemaphoreType.DMA((pieces,)),
            pltpu.SemaphoreType.DMA((pieces,)),
        ],
        input_output_aliases={8: 2},
        compiler_params=PARAMS,
        cost_estimate=cost(2 * K * tokens * chans, 8 << 20),
        name="taps_grad",
    )(conv, ng, stat, got2, gated, gg, swished, flat, pay3)
    after = lax.ppermute(head, "sp", back)
    got3 = lax.all_to_all(pay3, "sp", 0, 0, tiled=True)

    values_grad, gates_grad = pl.pallas_call(
        functools.partial(spread_kernel, blocks),
        grid=(seqs,),
        in_specs=[seq_block, head_block, seq_block, seq_block, whole((K, chans))],
        out_specs=[seq_block, seq_block],
        out_shape=[SDS((seqs, length, chans), BF16)] * 2,
        scratch_shapes=[pltpu.VMEM((length + 2 * PAD, chans), F32), pltpu.VMEM((PAD, chans), F32)],
        compiler_params=PARAMS,
        cost_estimate=cost(2 * K * tokens * chans, 8 << 20),
        name="gated_grad",
    )(cg, after, values_in, gates_in, conv_taps)

    weight_grad, taps_grad, gain_grad, bias_grad = pl.pallas_call(
        final_kernel,
        in_specs=[vmem],
        out_specs=[vmem] * 4,
        out_shape=[
            SDS((chans // sp, width), F32),
            SDS((K, chans), F32),
            SDS((1, chans), F32),
            SDS((1, chans), F32),
        ],
        compiler_params=PARAMS,
        name="final_sum",
    )(got3)
    gain_grad, bias_grad = gain_grad.reshape(chans), bias_grad.reshape(chans)
    return values_grad, gates_grad, taps_grad, gain_grad, bias_grad, weight_grad


def solution(mesh):
    return jax.shard_map(
        on_device,
        mesh=mesh,
        in_specs=(
            P(None, "sp", "tp"),
            P(None, "sp", "tp"),
            P(None, "tp"),
            P("tp"),
            P("tp"),
            P("tp", None),
            P(None, "sp", None),
        ),
        out_specs=(
            P(None, "sp", "tp"),
            P(None, "sp", "tp"),
            P(None, "tp"),
            P("tp"),
            P("tp"),
            P(("tp", "sp"), None),
        ),
        check_vma=False,
    )
```
